128 devices in a mesh: ep: 32 (over z, y, core), tp: 4 (over x).
Axes of the slice: x: 4, y: 4, z: 4, core: 2. Of those that a mesh axis runs over, the one named last changes fastest.
Arguments:
- tokens: bfloat16 [24576, 2048], P('ep')
- in_gain: float32 [2048], replicated, may hold values from 0.1 to 1.9
- route_ids: int32 [24576, 2], P('ep'), may hold values from 0 to 31, all different within a row; in each aligned block of 768 rows (0 to 767, 768 to 1535, ...) at most 96 rows name the same one
- route_scores: float32 [24576, 2], P('ep'), may hold values from 0.1 to 1
- gate_weight: bfloat16 [32, 2048, 1024], P('ep', None, 'tp'), may hold values from -0.125 to 0.125
- up_weight: bfloat16 [32, 2048, 1024], P('ep', None, 'tp'), may hold values from -0.125 to 0.125
- down_weight: bfloat16 [32, 1024, 2048], P('ep', 'tp')
- out_gain: float32 [2048], P('tp'), may hold values from 0.1 to 1.9
Outputs:
- mixed: bfloat16 [24576, 2048], P('ep', 'tp')
The draws below stay inside these ranges and needn't reach their ends.
Inputs may be any that keep to these rules, and one draw needn't show every extreme that they name: `route_ids`: each row names 2 different experts. Among the rows of one index of ep (aligned blocks of 768 rows) no expert is named more than 96 times, a bound that some block reaches.
All inputs are finite; a program needn't handle non-finite values.
Results may differ from the reference program's by a relative error of at most 0.012.
Values may be sent and summed in bfloat16 or wider, within the bound.
A program may use at most 128 MiB of HBM per device.

```python
import math
import jax
import jax.numpy as jnp
import numpy as np
from jax import lax

D = 2048
FF = 1024
TOP_K = 2
TOK_DEV = 768
EXPERTS = 32
TOKENS = 24576
CAP = 96
FF_PART = 256
N_EP = 32
N_TP = 4


def draw_tokens(key, part):
    keys = jax.random.split(jax.random.fold_in(key, 3), 3)
    row_scale = 10.0 ** jax.random.uniform(keys[1], (TOKENS, 1), jnp.float32)
    column_scale = 10.0 ** (0.5 * jax.random.uniform(keys[2], (1, D), jnp.float32))
    values = jax.random.normal(keys[0], (TOKENS, D), jnp.float32) * row_scale * column_scale
    return values.astype(jnp.bfloat16)


def draw_down_weight(key, part):
    keys = jax.random.split(jax.random.fold_in(key, 11), 2)
    position = jnp.arange(D, dtype=jnp.float32) / D
    base = jax.random.normal(keys[0], (EXPERTS, FF, D), jnp.float32)
    scale = 10.0 ** (0.5 * position + 0.5 * jax.random.uniform(keys[1], (D,), jnp.float32))
    return (base * FF ** (-0.5) * scale[None, None, :]).astype(jnp.bfloat16)


def steps_of(stream_key, dims, pieces, smallest, top_value):
    loudness = 1.0
    for dim, parts in pieces:
        draws = jax.random.uniform(jax.random.fold_in(jax.random.fold_in(stream_key, 6), dim), (parts,), jnp.float32, smallest / len(pieces), top_value / len(pieces))
        loudness = loudness * jnp.repeat(jnp.exp(draws), dims[dim] // parts).reshape((-1,) + (1,) * (len(dims) - 1 - dim))
    return loudness


def routed_block(own_key, own, number, rows, count, top, reach, lean):
    sequence = jax.random.permutation(own_key, count)
    crowded, usual = shares(count, rows * top, reach, lean, True), shares(count, rows * top, reach, lean, False)
    places = jnp.arange(count)

    def named(tallies, rotation):
        used = int((tallies > 0).sum())
        fixed = max(1, used // 4)
        moved = fixed + (places - fixed + rotation * (used - fixed)) % max(1, count - fixed)
        return jnp.zeros((count,), jnp.int32).at[sequence[jnp.where(places < fixed, places, moved)]].set(jnp.asarray(tallies, jnp.int32))

    tallies = jnp.where(number % 4 == 0, named(crowded, number // 4), named(usual, number - number // 4 - 1))
    mixed = jax.random.permutation(jax.random.fold_in(own, 3), count)
    giver, sink = mixed[0:count // 2 * 2:2], mixed[1:count // 2 * 2:2]
    margin = jnp.minimum(tallies[giver] - 1, reach - tallies[sink]) // 2
    margin = jnp.where((giver == sequence[0]) | (sink == sequence[0]) | (tallies[sink] == 0), 0, jnp.maximum(margin, 0))
    moved = jax.random.randint(jax.random.fold_in(own, 4), (count // 2,), 0, 1 << 20) % (margin + 1)
    tallies = tallies.at[giver].add(-moved).at[sink].add(moved)
    labels = jnp.searchsorted(jnp.cumsum(tallies), jnp.arange(rows * top), side="right").astype(jnp.int32)
    listing = labels.reshape(top, rows).T
    listing = listing[jax.random.permutation(jax.random.fold_in(own, 1), rows)]
    rotation = jax.random.randint(jax.random.fold_in(own, 2), (rows, 1), 0, top)
    return jnp.take_along_axis(listing, (jnp.arange(top)[None, :] + rotation) % top, axis=1)


def shares(count, total, most, slope, full):
    weights = [(1 << 20) // math.isqrt(standing ** slope) + 1 for standing in range(1, count + 1)]
    largest = most if full else min(most, max(-(-total // count), total * weights[0] // sum(weights)))
    least = 1 if total - largest >= count - 1 else 0
    counts, spare = [largest] + [least] * (count - 1), total - largest - least * (count - 1)
    while spare > 0:
        candidates = [i for i in range(1, count) if counts[i] < largest] or [i for i in range(1, count) if counts[i] < most]
        pool, left = sum([weights[i] for i in candidates]), spare
        for i in candidates:
            addition = min(most - counts[i], max(1, left * weights[i] // pool), spare)
            counts[i] = counts[i] + addition
            spare = spare - addition
    return np.array(counts)


def noise(stream_key, shape, scale, most, cuts=(), kind=jnp.bfloat16):
    values = scale * jax.random.normal(stream_key, shape, jnp.float32)
    if cuts:
        values = values * steps_of(stream_key, shape, cuts, -0.22, 0.18)
    return jnp.clip(values, -most, most).astype(kind)


def setup_inputs(seed: int = 0) -> dict:
    key_of = jax.random.split(jax.random.key(seed), 9)
    tokens = draw_tokens(jax.random.fold_in(key_of[8], 71), 0)
    in_gain = jnp.clip(1.0 + 0.18 * jax.random.normal(key_of[1], (D,), jnp.float32), 0.1, 1.9)
    route_ids_keys = jax.random.split(jax.random.fold_in(key_of[2], 1), TOKENS // TOK_DEV)
    route_ids_turns = jax.random.permutation(jax.random.fold_in(key_of[2], 3), TOKENS // TOK_DEV)
    route_ids = jax.vmap(lambda own, number: routed_block(jax.random.fold_in(key_of[2], 2), own, number, TOK_DEV, EXPERTS, TOP_K, CAP, 2))(route_ids_keys, route_ids_turns).reshape((TOKENS, TOP_K))
    route_scores = jnp.clip(jnp.exp(math.log(1.0) - 2.3025851 * jax.random.uniform(key_of[3], (TOKENS, TOP_K), jnp.float32) ** steps_of(key_of[3], (TOKENS, TOP_K), ((0, 32),), -0.2, 0.2)), 0.1, 1.0)
    gate_weight = noise(key_of[4], (EXPERTS, D, FF), D ** -0.5, 0.125, ((0, 32), (2, 4)))
    up_weight = noise(key_of[5], (EXPERTS, D, FF), D ** -0.5, 0.125, ((0, 32), (2, 4)))
    down_weight = draw_down_weight(jax.random.fold_in(key_of[8], 71), 0)
    out_gain = jnp.clip(1.0 + 0.18 * jax.random.normal(key_of[7], (D,), jnp.float32), 0.1, 1.9)
    return dict(tokens=tokens, in_gain=in_gain, route_ids=route_ids, route_scores=route_scores, gate_weight=gate_weight, up_weight=up_weight, down_weight=down_weight, out_gain=out_gain)


epsilon = 1e-06

def reference(tokens, in_gain, route_ids, route_scores, gate_weight, up_weight, down_weight, out_gain):
    as_float = tokens.astype(jnp.float32)
    normed = (as_float * lax.rsqrt(lax.optimization_barrier(jnp.mean(as_float * as_float, axis=1, keepdims=True)) + epsilon) * in_gain).astype(jnp.bfloat16)
    flat_ids = route_ids.reshape(N_EP, TOK_DEV * TOP_K)
    one_hot = (flat_ids[:, :, None] == jnp.arange(EXPERTS, dtype=jnp.int32)[None, None, :]).astype(jnp.int32)
    slot_index = lax.optimization_barrier(jnp.sum((jnp.cumsum(one_hot, axis=1) - 1) * one_hot, axis=2)).astype(jnp.int32)
    block_index = jnp.broadcast_to(jnp.arange(N_EP, dtype=jnp.int32)[:, None], flat_ids.shape)
    row_index = (block_index * TOK_DEV + jnp.arange(TOK_DEV * TOP_K, dtype=jnp.int32)[None, :] // TOP_K).astype(jnp.int32)
    buffer = jnp.zeros((EXPERTS, N_EP, CAP, D), jnp.bfloat16)
    buffer = buffer.at[flat_ids, block_index, slot_index].set(normed[row_index])

    def expert_run(inputs):
        rows_in, gate_w, up_w, down_w = inputs
        gate_acts = jnp.dot(rows_in, gate_w, preferred_element_type=jnp.float32)
        up_acts = jnp.dot(rows_in, up_w, preferred_element_type=jnp.float32)
        hidden = (jax.nn.silu(gate_acts) * up_acts).astype(jnp.bfloat16)
        hidden_blocks = hidden.reshape(-1, N_TP, FF_PART).astype(jnp.float32)
        down_blocks = down_w.reshape(N_TP, FF_PART, D).astype(jnp.float32)
        partial_value = jnp.einsum('rpf,pfd->prd', hidden_blocks, down_blocks)
        rounded = lax.optimization_barrier(partial_value.astype(jnp.bfloat16))
        return lax.optimization_barrier(jnp.sum(rounded.astype(jnp.float32), axis=0)).astype(jnp.bfloat16)
    outputs = lax.map(expert_run, (buffer.reshape(EXPERTS, N_EP * CAP, D), gate_weight, up_weight, down_weight))
    outputs = outputs.reshape(EXPERTS, N_EP, CAP, D)
    picked = outputs[flat_ids, block_index, slot_index].astype(jnp.float32).reshape(TOKENS, TOP_K, D)
    mix_weight = route_scores / lax.optimization_barrier(jnp.sum(route_scores, axis=1, keepdims=True))
    combined = lax.optimization_barrier(jnp.sum(mix_weight[:, :, None] * picked, axis=1))
    mixed = combined * lax.rsqrt(lax.optimization_barrier(jnp.mean(combined * combined, axis=1, keepdims=True)) + epsilon) * out_gain
    return mixed.astype(jnp.bfloat16)
```

```python
import jax
import jax.numpy as jnp
from jax import lax
from jax.experimental import pallas as pl
from jax.experimental.pallas import tpu as pltpu
from jax.sharding import PartitionSpec as P

EPS = 1e-06
MESH = pl.DeviceIdType.MESH
T = 768
D = 2048
F = 256
CAP = 96
HALF = 48
ROWS = 4 * 2 * HALF
DQ = 512
f32 = jnp.float32
bf16 = jnp.bfloat16


def dot(a, b):
    return jnp.dot(a, b, preferred_element_type=f32)


def at_rows(ref, start, size):
    return ref.at[pl.ds(pl.multiple_of(start, 16), size), :]


def kernel(
    tok_hbm, gain_ref, ids_ref, score_ref, wg_hbm, wu_hbm, wd_hbm, og_ref,
    out_ref,
    tok, s_buf, x_buf, wg, wu, wd, h_buf, h_recv, y_buf, r_buf,
    slot_t, onehot, sel, col0, col1, mix0, mix1, rowsum, comb, ns_buf, ns_recv,
    local_sem, s_send, x_recv, w_send, w_recv, h_send, h_rsem, y_send, r_recv, n_send, n_recv,
):
    ep = lax.axis_index("ep")
    x = lax.axis_index("tp")
    z = ep // 8
    y = (ep // 2) % 4
    c = ep % 2
    xs = (x - c + 5) % 4
    half = xs // 2
    member = xs % 2
    x_gate = ((((x - c + 4) % 4) + 1 - 2 * (((x - c + 4) % 4) % 2)) + c) % 4
    x_hid = (xs + 1 - 2 * member + c + 3) % 4
    x_far = (x + 2) % 4
    dm = (c + member) % 2

    def source_of(g, j, dc, sign):
        dy = (j + g + 1) % 4
        return (
            ((z + sign * j + 4) % 4) * 8 + ((y + sign * dy + 4) % 4) * 2 + (c + dc) % 2
        )

    tok_copy = pltpu.make_async_copy(tok_hbm, tok, local_sem.at[0])
    tok_copy.start()
    wg_copy = pltpu.make_async_copy(wg_hbm, wg.at[0], local_sem.at[1])
    wu_copy = pltpu.make_async_copy(wu_hbm, wu.at[0], local_sem.at[2])
    wd_copy = pltpu.make_async_copy(wd_hbm, wd.at[pl.ds(0, F), :], local_sem.at[3])
    wg_copy.start()
    wu_copy.start()
    wd_copy.start()

    barrier = pltpu.get_barrier_semaphore()

    def greet(i, _):
        d = (ep * 4 + x + i) % 128
        pl.semaphore_signal(barrier, inc=1, device_id=(d // 4, d % 4), device_id_type=MESH)
        return 0

    lax.fori_loop(1, 128, greet, 0)

    lanes = lax.broadcasted_iota(jnp.int32, (128, 128), 1)
    dz_l = ((lanes >> 3) - z) & 3
    dy_l = (((lanes >> 1) & 3) - y) & 3
    dc_l = ((lanes & 1) - c) & 1
    base = ((((dy_l - dz_l + 3) & 3) * 8 + dc_l * 4 + dz_l) * CAP).astype(f32)

    def mark(b, _):
        rows = pl.ds(pl.multiple_of(b * 128, 128), 128)
        ids = ids_ref[rows, :]
        named = (ids[:, 0:1] == lanes) | (ids[:, 1:2] == lanes)
        onehot[rows, :] = jnp.where(named, 1.0, 0.0).astype(bf16)
        return 0

    lax.fori_loop(0, 6, mark, 0)

    def number(b, _):
        rows = pl.ds(pl.multiple_of(b * 128, 128), 128)
        earlier = lax.broadcasted_iota(jnp.int32, (128, T), 1) < (
            lax.broadcasted_iota(jnp.int32, (128, T), 0) + b * 128
        )
        count = dot(jnp.where(earlier, 1.0, 0.0).astype(bf16), onehot[...])
        ids = ids_ref[rows, :]
        first = ids[:, 0:1] == lanes
        second = ids[:, 1:2] == lanes
        slot_t[:, rows] = jnp.where(first | second, count, -1.0).T
        place = count + base
        score = score_ref[rows, :]
        total = score[:, 0:1] + score[:, 1:2]
        col0[rows, :] = jnp.broadcast_to(
            jnp.sum(jnp.where(first, place, 0.0), axis=1, keepdims=True), (128, 128)
        )
        col1[rows, :] = jnp.broadcast_to(
            jnp.sum(jnp.where(second, place, 0.0), axis=1, keepdims=True), (128, 128)
        )
        mix0[rows, :] = jnp.broadcast_to(score[:, 0:1] / total, (128, 128))
        mix1[rows, :] = jnp.broadcast_to(score[:, 1:2] / total, (128, 128))
        return 0

    lax.fori_loop(0, 6, number, 0)

    tok_copy.wait()

    def squares(b, _):
        rows = pl.ds(pl.multiple_of(b * 64, 64), 64)
        acc = jnp.zeros((64, 128), f32)
        for q in range(16):
            v = tok[rows, q * 128 : (q + 1) * 128].astype(f32)
            acc = acc + v * v
        rowsum[rows, :] = acc
        return 0

    lax.fori_loop(0, 12, squares, 0)

    def scale_of(b, _):
        rows = pl.ds(pl.multiple_of(b * 256, 256), 256)
        mean = jnp.sum(rowsum[rows, :], axis=1, keepdims=True) * (1.0 / D)
        rowsum[rows, :] = jnp.broadcast_to(lax.rsqrt(mean + EPS), (256, 128))
        return 0

    lax.fori_loop(0, 3, scale_of, 0)

    def normalize(b, _):
        rows = pl.ds(pl.multiple_of(b * 64, 64), 64)
        scale = rowsum[rows, :]
        for q in range(16):
            cols = slice(q * 128, (q + 1) * 128)
            v = tok[rows, cols].astype(f32) * scale * gain_ref[:, cols]
            tok[rows, cols] = v.astype(bf16)
        return 0

    lax.fori_loop(0, 12, normalize, 0)

    def pack(g, _):
        for q in range(8):
            dc, j = q // 4, q % 4
            e = source_of(g, j, dc, 1)
            first = ((x - (c + dc) % 2 + 5) % 4) // 2 * HALF
            want = lax.broadcasted_iota(jnp.int32, (HALF, T), 0) + first
            row = slot_t[pl.ds(e, 1), :]
            sel[q * HALF : (q + 1) * HALF, :] = jnp.where(
                row == want.astype(f32), 1.0, 0.0
            ).astype(bf16)
        rows = pl.ds(pl.multiple_of(g * ROWS, ROWS), ROWS)

        def part(n, _):
            cols = pl.ds(pl.multiple_of(n * 512, 512), 512)
            s_buf[rows, cols] = dot(sel[0:ROWS, :], tok[:, cols]).astype(bf16)
            return 0

        lax.fori_loop(0, 4, part, 0)
        return 0

    lax.fori_loop(0, 4, pack, 0)
    own = slice(24 * HALF, 25 * HALF)
    x_buf[own, :] = s_buf[own, :]

    pl.semaphore_wait(barrier, 127)

    def send_weight(src, dst, to, sem):
        cp = pltpu.make_async_remote_copy(
            src_ref=src, dst_ref=dst, send_sem=w_send.at[sem], recv_sem=w_recv.at[sem],
            device_id=(ep, to), device_id_type=MESH,
        )
        cp.start()
        return cp

    w_copies = [
        send_weight(wg_hbm, wg.at[1], x_gate, 0),
        send_weight(wu_hbm, wu.at[1], x_gate, 1),
        send_weight(wd_hbm, wd.at[pl.ds(2 * F, F), :], x_hid, 2),
        send_weight(wd_hbm, wd.at[pl.ds(F, F), :], x_gate, 3),
        send_weight(wd_hbm, wd.at[pl.ds(3 * F, F), :], x_far, 4),
    ]

    def dispatch(g, _):
        def one(q, _):
            k, dc, j = q // 8, (q // 4) % 2, q % 4

            @pl.when(jnp.logical_or(g < 3, q % 8 > 0))
            def _():
                row = (g * 8 + q % 8) * HALF + k * 16
                pltpu.make_async_remote_copy(
                    src_ref=at_rows(s_buf, row, 16), dst_ref=at_rows(x_buf, row, 16),
                    send_sem=s_send, recv_sem=x_recv.at[g],
                    device_id=(source_of(g, j, dc, 1), x), device_id_type=MESH,
                ).start()

            return 0

        lax.fori_loop(0, 24, one, 0)
        return 0

    lax.fori_loop(0, 4, dispatch, 0)

    def arrived(ref, rows, sem):
        part = ref.at[pl.ds(0, rows), :]
        pltpu.make_async_copy(part, part, sem).wait()

    wg_copy.wait()
    wu_copy.wait()
    wd_copy.wait()
    for cp in w_copies[:2]:
        cp.wait()

    def expert(g, _):
        @pl.when(g < 3)
        def _():
            arrived(x_buf, ROWS, x_recv.at[g])

        @pl.when(g == 3)
        def _():
            arrived(x_buf, ROWS - HALF, x_recv.at[g])

        rows = pl.ds(pl.multiple_of(g * ROWS, ROWS), ROWS)
        for k in range(2):
            gate = dot(x_buf[rows, :], wg[k])
            up = dot(x_buf[rows, :], wu[k])
            hid = (gate / (1.0 + jnp.exp(-gate)) * up).astype(bf16)
            h_buf[g * 2, :, k * F : (k + 1) * F] = hid[: ROWS // 2]
            h_buf[g * 2 + 1, :, k * F : (k + 1) * F] = hid[ROWS // 2 :]
        cp = pltpu.make_async_remote_copy(
            src_ref=h_buf.at[g * 2 + 1 - dm], dst_ref=h_recv.at[g],
            send_sem=h_send.at[g], recv_sem=h_rsem.at[g],
            device_id=(ep, x_hid), device_id_type=MESH,
        )
        cp.start()

        @pl.when(g == 0)
        def _():
            for late in w_copies[2:]:
                late.wait()

        cp.wait()

        def down(q, _):
            cols = pl.ds(pl.multiple_of(q * DQ, DQ), DQ)
            v = dot(h_buf[g * 2 + dm], wd[0 : 2 * F, cols])
            v = v + dot(h_recv[g], wd[2 * F : 4 * F, cols])
            y_buf[pl.ds(pl.multiple_of((g * 4 + q) * ROWS // 2, ROWS // 2), ROWS // 2), :] = (
                v.astype(bf16)
            )
            return 0

        lax.fori_loop(0, 4, down, 0)

        def give(q, _):
            j = q % 4
            to = (x + q // 4 + j) % 4
            src = ((g * 4 + to) * 4 + j) * HALF
            dst = ((g * 8 + dm * 4 + j) * 2 + half) * HALF
            mine = (g == 3) & (j == 0) & (dm == 0) & (to == x)

            @pl.when(jnp.logical_not(mine))
            def _():
                pltpu.make_async_remote_copy(
                    src_ref=at_rows(y_buf, src, HALF), dst_ref=at_rows(r_buf, dst, HALF),
                    send_sem=y_send, recv_sem=r_recv.at[g],
                    device_id=(source_of(g, j, dm, -1), to), device_id_type=MESH,
                ).start()

            return 0

        lax.fori_loop(0, 16, give, 0)
        return 0

    lax.fori_loop(0, 4, expert, 0)

    @pl.when(dm == 0)
    def _():
        src = pl.ds(pl.multiple_of((12 + x) * 4 * HALF, 16), HALF)
        dst = pl.ds(pl.multiple_of((48 + half) * HALF, 16), HALF)
        r_buf[dst, :] = y_buf[src, :]

    comb[...] = jnp.zeros_like(comb)

    def combine(g, _):
        def weigh(b, _):
            rows = pl.ds(pl.multiple_of(b * 128, 128), 128)
            for q in range(6):
                here = (lanes + (g * 8 * CAP + q * 128)).astype(f32)
                v = jnp.where(col0[rows, :] == here, mix0[rows, :], 0.0)
                v = v + jnp.where(col1[rows, :] == here, mix1[rows, :], 0.0)
                sel[rows, q * 128 : (q + 1) * 128] = v.astype(bf16)
            return 0

        lax.fori_loop(0, 6, weigh, 0)

        @pl.when(jnp.logical_or(g < 3, dm == 1))
        def _():
            arrived(r_buf, 16 * HALF, r_recv.at[g])

        @pl.when(jnp.logical_and(g == 3, dm == 0))
        def _():
            arrived(r_buf, 15 * HALF, r_recv.at[g])

        rows = pl.ds(pl.multiple_of(g * 8 * CAP, 8 * CAP), 8 * CAP)
        comb[...] += dot(sel[...], r_buf[rows, :])
        return 0

    lax.fori_loop(0, 4, combine, 0)

    def square_sum(b, _):
        rows = pl.ds(pl.multiple_of(b * 128, 128), 128)
        acc = jnp.zeros((128, 128), f32)
        for q in range(4):
            v = comb[rows, q * 128 : (q + 1) * 128]
            acc = acc + v * v
        ns_buf[:, rows] = jnp.sum(acc.T.reshape(16, 8, 128), axis=0)
        return 0

    lax.fori_loop(0, 6, square_sum, 0)
    n_copies = []
    for d in range(1, 4):
        cp = pltpu.make_async_remote_copy(
            src_ref=ns_buf, dst_ref=ns_recv.at[d - 1], send_sem=n_send.at[d - 1],
            recv_sem=n_recv.at[d - 1], device_id=(ep, (x + d) % 4), device_id_type=MESH,
        )
        cp.start()
        n_copies.append(cp)
    for cp in n_copies:
        cp.wait()

    def finish(b, _):
        rows = pl.ds(pl.multiple_of(b * 128, 128), 128)
        total = ns_buf[:, rows] + ns_recv[0, :, rows] + ns_recv[1, :, rows] + ns_recv[2, :, rows]
        total = jnp.sum(total, axis=0, keepdims=True)
        scale = lax.rsqrt(total * (1.0 / D) + EPS)
        scale = jnp.broadcast_to(scale, (128, 128)).T
        for q in range(4):
            cols = slice(q * 128, (q + 1) * 128)
            out_ref[rows, cols] = (comb[rows, cols] * scale * og_ref[:, cols]).astype(bf16)
        return 0

    lax.fori_loop(0, 6, finish, 0)

    arrived(s_buf, 31 * HALF, s_send)

    @pl.when(dm == 0)
    def _():
        arrived(y_buf, 63 * HALF, y_send)

    @pl.when(dm == 1)
    def _():
        arrived(y_buf, 64 * HALF, y_send)


def per_device(
    tokens, in_gain, route_ids, route_scores, gate_weight, up_weight, down_weight, out_gain
):
    vmem = pl.BlockSpec(memory_space=pltpu.VMEM)
    hbm = pl.BlockSpec(memory_space=pl.ANY)
    dma = pltpu.SemaphoreType.DMA
    return pl.pallas_call(
        kernel,
        out_shape=jax.ShapeDtypeStruct((T, DQ), bf16),
        in_specs=[hbm, vmem, vmem, vmem, hbm, hbm, hbm, vmem],
        out_specs=vmem,
        scratch_shapes=[
            pltpu.VMEM((T, D), bf16),
            pltpu.VMEM((4 * ROWS, D), bf16),
            pltpu.VMEM((4 * ROWS, D), bf16),
            pltpu.VMEM((2, D, F), bf16),
            pltpu.VMEM((2, D, F), bf16),
            pltpu.VMEM((4 * F, D), bf16),
            pltpu.VMEM((8, ROWS // 2, 2 * F), bf16),
            pltpu.VMEM((4, ROWS // 2, 2 * F), bf16),
            pltpu.VMEM((64 * HALF, DQ), bf16),
            pltpu.VMEM((64 * HALF, DQ), bf16),
            pltpu.VMEM((128, T), f32),
            pltpu.VMEM((T, 128), bf16),
            pltpu.VMEM((T, T), bf16),
            pltpu.VMEM((T, 128), f32),
            pltpu.VMEM((T, 128), f32),
            pltpu.VMEM((T, 128), f32),
            pltpu.VMEM((T, 128), f32),
            pltpu.VMEM((T, 128), f32),
            pltpu.VMEM((T, DQ), f32),
            pltpu.VMEM((8, T), f32),
            pltpu.VMEM((3, 8, T), f32),
            dma((4,)),
            dma,
            dma((4,)),
            dma((5,)),
            dma((5,)),
            dma((4,)),
            dma((4,)),
            dma,
            dma((4,)),
            dma((3,)),
            dma((3,)),
        ],
        compiler_params=pltpu.CompilerParams(
            collective_id=0, has_side_effects=True, vmem_limit_bytes=62 * 2**20
        ),
        name="routed_experts",
    )(
        tokens,
        in_gain.reshape(1, D),
        route_ids,
        route_scores,
        gate_weight.reshape(D, F),
        up_weight.reshape(D, F),
        down_weight.reshape(F, D),
        out_gain.reshape(1, DQ),
    )


def solution(mesh):
    in_specs = (
        P("ep", None),
        P(),
        P("ep", None),
        P("ep", None),
        P("ep", None, "tp"),
        P("ep", None, "tp"),
        P("ep", "tp", None),
        P("tp"),
    )
    return jax.shard_map(
        per_device, mesh=mesh, in_specs=in_specs, out_specs=P("ep", "tp"), check_vma=False
    )
```

```python
import jax
import jax.numpy as jnp
from jax import lax
from jax.experimental import pallas as pl
from jax.experimental.pallas import tpu as pltpu
from jax.sharding import PartitionSpec as P

EPS = 1e-06
MESH = pl.DeviceIdType.MESH
T = 768
D = 2048
F = 256
CAP = 96
HALF = 48
ROWS = 4 * 2 * HALF
DQ = 512
f32 = jnp.float32
bf16 = jnp.bfloat16


def dot(a, b):
    return jnp.dot(a, b, preferred_element_type=f32)


def at_rows(ref, start, size):
    return ref.at[pl.ds(pl.multiple_of(start, 16), size), :]


def kernel(
    tok_hbm, gain_ref, ids_ref, score_ref, wg_hbm, wu_hbm, wd_hbm, og_ref,
    out_ref,
    tok, s_buf, x_buf, wg, wu, wd, h_buf, h_recv, y_buf, r_buf,
    slot_t, onehot, sel, col0, col1, mix0, mix1, rowsum, comb, ns_buf, ns_recv,
    local_sem, s_send, x_recv, w_send, w_recv, h_send, h_rsem, y_send, r_recv, n_send, n_recv, ready,
):
    ep = lax.axis_index("ep")
    x = lax.axis_index("tp")
    z = ep // 8
    y = (ep // 2) % 4
    c = ep % 2
    xs = (x - c + 5) % 4
    half = xs // 2
    member = xs % 2
    x_gate = ((((x - c + 4) % 4) + 1 - 2 * (((x - c + 4) % 4) % 2)) + c) % 4
    x_hid = (xs + 1 - 2 * member + c + 3) % 4
    x_far = (x + 2) % 4
    dm = (c + member) % 2

    def source_of(g, j, dc, sign):
        dy = (j + g + 1) % 4
        return (
            ((z + sign * j + 4) % 4) * 8 + ((y + sign * dy + 4) % 4) * 2 + (c + dc) % 2
        )

    tok_copy = pltpu.make_async_copy(tok_hbm, tok, local_sem.at[0])
    tok_copy.start()
    wg_copy = pltpu.make_async_copy(wg_hbm, wg.at[0], local_sem.at[1])
    wu_copy = pltpu.make_async_copy(wu_hbm, wu.at[0], local_sem.at[2])
    wd_copy = pltpu.make_async_copy(wd_hbm, wd.at[pl.ds(0, F), :], local_sem.at[3])
    wg_copy.start()
    wu_copy.start()
    wd_copy.start()

    barrier = pltpu.get_barrier_semaphore()

    def greet(i, _):
        pl.semaphore_signal(
            barrier, inc=1, device_id=((ep + i) % 32, x), device_id_type=MESH
        )
        return 0

    lax.fori_loop(1, 32, greet, 0)
    for d in range(1, 4):
        pl.semaphore_signal(
            barrier, inc=1, device_id=(ep, (x + d) % 4), device_id_type=MESH
        )

    lanes = lax.broadcasted_iota(jnp.int32, (128, 128), 1)
    dz_l = ((lanes >> 3) - z) & 3
    dy_l = (((lanes >> 1) & 3) - y) & 3
    dc_l = ((lanes & 1) - c) & 1
    base = ((((dy_l - dz_l + 3) & 3) * 8 + dc_l * 4 + dz_l) * CAP).astype(f32)

    lanes_f = lanes.astype(f32)

    def column(row):
        return jnp.broadcast_to(row, (128, 128)).T

    def mark(b, _):
        rows = pl.ds(pl.multiple_of(b * 128, 128), 128)
        first = column(ids_ref[0:1, rows].astype(f32))
        second = column(ids_ref[1:2, rows].astype(f32))
        col0[rows, :] = first
        col1[rows, :] = second
        named = (first == lanes_f) | (second == lanes_f)
        onehot[rows, :] = jnp.where(named, 1.0, 0.0).astype(bf16)
        score0 = score_ref[0:1, rows]
        score1 = score_ref[1:2, rows]
        mix0[rows, :] = column(score0 / (score0 + score1))
        mix1[rows, :] = column(score1 / (score0 + score1))
        return 0

    lax.fori_loop(0, 6, mark, 0)

    def number(b, _):
        rows = pl.ds(pl.multiple_of(b * 128, 128), 128)
        earlier = lax.broadcasted_iota(jnp.int32, (128, T), 1) < (
            lax.broadcasted_iota(jnp.int32, (128, T), 0) + b * 128
        )
        count = dot(jnp.where(earlier, 1.0, 0.0).astype(bf16), onehot[...])
        first = col0[rows, :] == lanes_f
        second = col1[rows, :] == lanes_f
        slot_t[:, rows] = jnp.where(first | second, count, -1.0).T
        place = count + base
        col0[rows, :] = jnp.broadcast_to(
            jnp.sum(jnp.where(first, place, 0.0), axis=1, keepdims=True), (128, 128)
        )
        col1[rows, :] = jnp.broadcast_to(
            jnp.sum(jnp.where(second, place, 0.0), axis=1, keepdims=True), (128, 128)
        )
        return 0

    lax.fori_loop(0, 6, number, 0)

    tok_copy.wait()

    def squares(b, _):
        rows = pl.ds(pl.multiple_of(b * 64, 64), 64)
        acc = jnp.zeros((64, 128), f32)
        for q in range(16):
            v = tok[rows, q * 128 : (q + 1) * 128].astype(f32)
            acc = acc + v * v
        rowsum[rows, :] = acc
        return 0

    lax.fori_loop(0, 12, squares, 0)

    def scale_of(b, _):
        rows = pl.ds(pl.multiple_of(b * 256, 256), 256)
        mean = jnp.sum(rowsum[rows, :], axis=1, keepdims=True) * (1.0 / D)
        rowsum[rows, :] = jnp.broadcast_to(lax.rsqrt(mean + EPS), (256, 128))
        return 0

    lax.fori_loop(0, 3, scale_of, 0)

    def normalize(b, _):
        rows = pl.ds(pl.multiple_of(b * 64, 64), 64)
        scale = rowsum[rows, :]
        for q in range(16):
            cols = slice(q * 128, (q + 1) * 128)
            v = tok[rows, cols].astype(f32) * scale * gain_ref[:, cols]
            tok[rows, cols] = v.astype(bf16)
        return 0

    lax.fori_loop(0, 12, normalize, 0)

    def pack(g, _):
        for q in range(8):
            dc, j = q // 4, q % 4
            e = source_of(g, j, dc, 1)
            first = ((x - (c + dc) % 2 + 5) % 4) // 2 * HALF
            want = lax.broadcasted_iota(jnp.int32, (HALF, T), 0) + first
            row = slot_t[pl.ds(e, 1), :]
            sel[q * HALF : (q + 1) * HALF, :] = jnp.where(
                row == want.astype(f32), 1.0, 0.0
            ).astype(bf16)
        rows = pl.ds(pl.multiple_of(g * ROWS, ROWS), ROWS)

        def part(n, _):
            cols = pl.ds(pl.multiple_of(n * 512, 512), 512)
            s_buf[rows, cols] = dot(sel[0:ROWS, :], tok[:, cols]).astype(bf16)
            return 0

        lax.fori_loop(0, 4, part, 0)
        return 0

    def dispatch(g, _):
        def one(q, _):
            k, dc, j = q // 8, (q // 4) % 2, q % 4

            @pl.when(jnp.logical_or(g < 3, q % 8 > 0))
            def _():
                row = (g * 8 + q % 8) * HALF + k * 16
                pltpu.make_async_remote_copy(
                    src_ref=at_rows(s_buf, row, 16), dst_ref=at_rows(x_buf, row, 16),
                    send_sem=s_send, recv_sem=x_recv.at[g],
                    device_id=(source_of(g, j, dc, 1), x), device_id_type=MESH,
                ).start()

            return 0

        lax.fori_loop(0, 24, one, 0)
        return 0

    def send_weight(src, dst, to, sem):
        cp = pltpu.make_async_remote_copy(
            src_ref=src, dst_ref=dst, send_sem=w_send.at[sem], recv_sem=w_recv.at[sem],
            device_id=(ep, to), device_id_type=MESH,
        )
        cp.start()
        return cp

    def shard(k, lo=0, size=F):
        return wd.at[pl.ds(k * F + lo, size), :]

    pack(0, 0)
    pl.semaphore_wait(barrier, 34)
    w_copies = [
        send_weight(wg_hbm, wg.at[1], x_gate, 0),
        send_weight(wu_hbm, wu.at[1], x_gate, 1),
        send_weight(wd_hbm, shard(2), x_hid, 2),
        send_weight(wd_hbm, shard(1), x_gate, 3),
    ]
    dispatch(0, 0)
    for d in range(1, 4):
        pl.semaphore_signal(
            ready, inc=1, device_id=(ep, (x + d) % 4), device_id_type=MESH
        )

    def pack_and_send(g, _):
        pack(g, 0)
        dispatch(g, 0)
        return 0

    lax.fori_loop(1, 4, pack_and_send, 0)
    own = slice(24 * HALF, 25 * HALF)
    x_buf[own, :] = s_buf[own, :]

    def arrived(ref, rows, sem):
        part = ref.at[pl.ds(0, rows), :]
        pltpu.make_async_copy(part, part, sem).wait()

    wg_copy.wait()
    wu_copy.wait()
    wd_copy.wait()
    for cp in w_copies[:2]:
        cp.wait()

    def swap(g):
        return pltpu.make_async_remote_copy(
            src_ref=h_buf.at[g * 2 + 1 - dm], dst_ref=h_recv.at[g],
            send_sem=h_send.at[g], recv_sem=h_rsem.at[g],
            device_id=(ep, x_hid), device_id_type=MESH,
        )

    def hidden(g):
        for side in (1 - dm, dm):
            rows = pl.ds(pl.multiple_of((g * 2 + side) * (ROWS // 2), ROWS // 2), ROWS // 2)
            for k in range(2):
                gate = dot(x_buf[rows, :], wg[k])
                up = dot(x_buf[rows, :], wu[k])
                h_buf[g * 2 + side, :, k * F : (k + 1) * F] = (
                    gate / (1.0 + jnp.exp(-gate)) * up
                ).astype(bf16)
            if side is not dm:
                swap(g).start()

    def down(g):
        swap(g).wait()

        def part(q, _):
            cols = pl.ds(pl.multiple_of(q * DQ, DQ), DQ)
            v = dot(h_buf[g * 2 + dm], wd[0 : 2 * F, cols])
            v = v + dot(h_recv[g], wd[2 * F : 4 * F, cols])
            y_buf[pl.ds(pl.multiple_of((g * 4 + q) * ROWS // 2, ROWS // 2), ROWS // 2), :] = (
                v.astype(bf16)
            )
            return 0

        lax.fori_loop(0, 4, part, 0)

    def give(g):
        def one(q, _):
            j = q % 4
            to = (x + q // 4 + j) % 4
            src = ((g * 4 + to) * 4 + j) * HALF
            dst = ((g * 8 + dm * 4 + j) * 2 + half) * HALF
            mine = (g == 3) & (j == 0) & (dm == 0) & (to == x)

            @pl.when(jnp.logical_not(mine))
            def _():
                pltpu.make_async_remote_copy(
                    src_ref=at_rows(y_buf, src, HALF), dst_ref=at_rows(r_buf, dst, HALF),
                    send_sem=y_send, recv_sem=r_recv.at[g],
                    device_id=(source_of(g, j, dm, -1), to), device_id_type=MESH,
                ).start()

            return 0

        lax.fori_loop(0, 16, one, 0)

    def expert(g, _):
        @pl.when(g < 3)
        def _():
            arrived(x_buf, ROWS, x_recv.at[g])

        @pl.when(g == 3)
        def _():
            arrived(x_buf, ROWS - HALF, x_recv.at[g])

        hidden(g)

        @pl.when(g == 1)
        def _():
            w_copies[2].wait()
            send_weight(shard(2, 0, F // 2), shard(3, 0, F // 2), x_gate, 4)
            w_copies[3].wait()
            send_weight(shard(1, F // 2, F // 2), shard(3, F // 2, F // 2), x_hid, 5)

        @pl.when(g == 2)
        def _():
            for k in (4, 5):
                pltpu.make_async_remote_copy(
                    src_ref=shard(1, 0, F // 2), dst_ref=shard(3, (k - 4) * (F // 2), F // 2),
                    send_sem=w_send.at[k], recv_sem=w_recv.at[k],
                    device_id=(ep, x_hid), device_id_type=MESH,
                ).wait()
            pl.semaphore_wait(ready, 3)

            def early(i, _):
                down(i)

                @pl.when(i == 0)
                def _():
                    give(0)

                return 0

            lax.fori_loop(0, 3, early, 0)

        @pl.when(g == 3)
        def _():
            give(1)
            give(2)
            down(3)
            give(3)

        return 0

    lax.fori_loop(0, 4, expert, 0)

    @pl.when(dm == 0)
    def _():
        src = pl.ds(pl.multiple_of((12 + x) * 4 * HALF, 16), HALF)
        dst = pl.ds(pl.multiple_of((48 + half) * HALF, 16), HALF)
        r_buf[dst, :] = y_buf[src, :]

    comb[...] = jnp.zeros_like(comb)

    def combine(g, _):
        def weigh(b, _):
            rows = pl.ds(pl.multiple_of(b * 128, 128), 128)
            for q in range(6):
                here = (lanes + (g * 8 * CAP + q * 128)).astype(f32)
                v = jnp.where(col0[rows, :] == here, mix0[rows, :], 0.0)
                v = v + jnp.where(col1[rows, :] == here, mix1[rows, :], 0.0)
                sel[rows, q * 128 : (q + 1) * 128] = v.astype(bf16)
            return 0

        lax.fori_loop(0, 6, weigh, 0)

        @pl.when(jnp.logical_or(g < 3, dm == 1))
        def _():
            arrived(r_buf, 16 * HALF, r_recv.at[g])

        @pl.when(jnp.logical_and(g == 3, dm == 0))
        def _():
            arrived(r_buf, 15 * HALF, r_recv.at[g])

        rows = pl.ds(pl.multiple_of(g * 8 * CAP, 8 * CAP), 8 * CAP)
        comb[...] += dot(sel[...], r_buf[rows, :])
        return 0

    lax.fori_loop(0, 4, combine, 0)

    def square_sum(b, _):
        rows = pl.ds(pl.multiple_of(b * 128, 128), 128)
        acc = jnp.zeros((128, 128), f32)
        for q in range(4):
            v = comb[rows, q * 128 : (q + 1) * 128]
            acc = acc + v * v
        ns_buf[:, rows] = jnp.sum(acc.T.reshape(16, 8, 128), axis=0)
        return 0

    lax.fori_loop(0, 6, square_sum, 0)
    n_copies = []
    for d in range(1, 4):
        cp = pltpu.make_async_remote_copy(
            src_ref=ns_buf, dst_ref=ns_recv.at[d - 1], send_sem=n_send.at[d - 1],
            recv_sem=n_recv.at[d - 1], device_id=(ep, (x + d) % 4), device_id_type=MESH,
        )
        cp.start()
        n_copies.append(cp)
    for cp in n_copies:
        cp.wait()

    def finish(b, _):
        rows = pl.ds(pl.multiple_of(b * 128, 128), 128)
        total = ns_buf[:, rows] + ns_recv[0, :, rows] + ns_recv[1, :, rows] + ns_recv[2, :, rows]
        total = jnp.sum(total, axis=0, keepdims=True)
        scale = lax.rsqrt(total * (1.0 / D) + EPS)
        scale = jnp.broadcast_to(scale, (128, 128)).T
        for q in range(4):
            cols = slice(q * 128, (q + 1) * 128)
            out_ref[rows, cols] = (comb[rows, cols] * scale * og_ref[:, cols]).astype(bf16)
        return 0

    lax.fori_loop(0, 6, finish, 0)

    arrived(s_buf, 31 * HALF, s_send)

    @pl.when(dm == 0)
    def _():
        arrived(y_buf, 63 * HALF, y_send)

    @pl.when(dm == 1)
    def _():
        arrived(y_buf, 64 * HALF, y_send)


def per_device(
    tokens, in_gain, route_ids, route_scores, gate_weight, up_weight, down_weight, out_gain
):
    vmem = pl.BlockSpec(memory_space=pltpu.VMEM)
    hbm = pl.BlockSpec(memory_space=pl.ANY)
    dma = pltpu.SemaphoreType.DMA
    return pl.pallas_call(
        kernel,
        out_shape=jax.ShapeDtypeStruct((T, DQ), bf16),
        in_specs=[hbm, vmem, vmem, vmem, hbm, hbm, hbm, vmem],
        out_specs=vmem,
        scratch_shapes=[
            pltpu.VMEM((T, D), bf16),
            pltpu.VMEM((4 * ROWS, D), bf16),
            pltpu.VMEM((4 * ROWS, D), bf16),
            pltpu.VMEM((2, D, F), bf16),
            pltpu.VMEM((2, D, F), bf16),
            pltpu.VMEM((4 * F, D), bf16),
            pltpu.VMEM((8, ROWS // 2, 2 * F), bf16),
            pltpu.VMEM((4, ROWS // 2, 2 * F), bf16),
            pltpu.VMEM((64 * HALF, DQ), bf16),
            pltpu.VMEM((64 * HALF, DQ), bf16),
            pltpu.VMEM((128, T), f32),
            pltpu.VMEM((T, 128), bf16),
            pltpu.VMEM((T, T), bf16),
            pltpu.VMEM((T, 128), f32),
            pltpu.VMEM((T, 128), f32),
            pltpu.VMEM((T, 128), f32),
            pltpu.VMEM((T, 128), f32),
            pltpu.VMEM((T, 128), f32),
            pltpu.VMEM((T, DQ), f32),
            pltpu.VMEM((8, T), f32),
            pltpu.VMEM((3, 8, T), f32),
            dma((4,)),
            dma,
            dma((4,)),
            dma((6,)),
            dma((6,)),
            dma((4,)),
            dma((4,)),
            dma,
            dma((4,)),
            dma((3,)),
            dma((3,)),
            pltpu.SemaphoreType.REGULAR,
        ],
        compiler_params=pltpu.CompilerParams(
            collective_id=0, has_side_effects=True, vmem_limit_bytes=62 * 2**20
        ),
        name="routed_experts",
    )(
        tokens,
        in_gain.reshape(1, D),
        route_ids.T,
        route_scores.T,
        gate_weight.reshape(D, F),
        up_weight.reshape(D, F),
        down_weight.reshape(F, D),
        out_gain.reshape(1, DQ),
    )


def solution(mesh):
    in_specs = (
        P("ep", None),
        P(),
        P("ep", None),
        P("ep", None),
        P("ep", None, "tp"),
        P("ep", None, "tp"),
        P("ep", "tp", None),
        P("tp"),
    )
    return jax.shard_map(
        per_device, mesh=mesh, in_specs=in_specs, out_specs=P("ep", "tp"), check_vma=False
    )
```

```python
import jax
import jax.numpy as jnp
from jax import lax
from jax.experimental import pallas as pl
from jax.experimental.pallas import tpu as pltpu
from jax.sharding import PartitionSpec as P

EPS = 1e-06
MESH = pl.DeviceIdType.MESH
T = 768
D = 2048
F = 256
CAP = 96
HALF = 48
ROWS = 4 * 2 * HALF
DQ = 512
f32 = jnp.float32
bf16 = jnp.bfloat16


def dot(a, b):
    return jnp.dot(a, b, preferred_element_type=f32)


def at_rows(ref, start, size):
    return ref.at[pl.ds(pl.multiple_of(start, 16), size), :]


def kernel(
    tok_hbm, gain_ref, ids_ref, score_ref, wg_hbm, wu_hbm, wd_hbm, og_ref,
    out_ref,
    tok, s_buf, x_buf, wg, wu, wd, h_buf, h_recv, y_buf, r_buf,
    slot_t, onehot, sel, col0, col1, mix0, mix1, rowsum, comb, ns_buf, ns_recv,
    local_sem, s_send, x_recv, w_send, w_recv, h_send, h_rsem, y_send, r_recv, n_send, n_recv, ready,
):
    ep = lax.axis_index("ep")
    x = lax.axis_index("tp")
    z = ep // 8
    y = (ep // 2) % 4
    c = ep % 2
    xs = (x - c + 5) % 4
    half = xs // 2
    member = xs % 2
    x_gate = ((((x - c + 4) % 4) + 1 - 2 * (((x - c + 4) % 4) % 2)) + c) % 4
    x_hid = (xs + 1 - 2 * member + c + 3) % 4
    x_far = (x + 2) % 4

    def source_of(g, j, dc, sign):
        dy = (j + g + 1) % 4
        return (
            ((z + sign * j + 4) % 4) * 8 + ((y + sign * dy + 4) % 4) * 2 + (c + dc) % 2
        )

    tok_copy = pltpu.make_async_copy(tok_hbm, tok, local_sem.at[0])
    tok_copy.start()
    wg_copy = pltpu.make_async_copy(wg_hbm, wg.at[0], local_sem.at[1])
    wu_copy = pltpu.make_async_copy(wu_hbm, wu.at[0], local_sem.at[2])

    def features(k):
        return pl.ds(pl.multiple_of(k * DQ, DQ), DQ)

    def shard(k, part):
        return wd.at[pl.ds(k * F, F), pl.ds(part * DQ, DQ)]

    wd_copies = [
        pltpu.make_async_copy(wd_hbm.at[:, features(k)], shard(0, q), local_sem.at[3 + q])
        for q, k in enumerate((x, x_gate))
    ]
    wg_copy.start()
    wu_copy.start()
    for cp in wd_copies:
        cp.start()

    barrier = pltpu.get_barrier_semaphore()

    def greet(i, _):
        pl.semaphore_signal(
            barrier, inc=1, device_id=((ep + i) % 32, x), device_id_type=MESH
        )
        return 0

    lax.fori_loop(1, 32, greet, 0)
    for d in range(1, 4):
        pl.semaphore_signal(
            barrier, inc=1, device_id=(ep, (x + d) % 4), device_id_type=MESH
        )

    lanes = lax.broadcasted_iota(jnp.int32, (128, 128), 1)
    dz_l = ((lanes >> 3) - z) & 3
    dy_l = (((lanes >> 1) & 3) - y) & 3
    dc_l = ((lanes & 1) - c) & 1
    base = ((((dy_l - dz_l + 3) & 3) * 8 + dc_l * 4 + dz_l) * CAP).astype(f32)

    lanes_f = lanes.astype(f32)

    def column(row):
        return jnp.broadcast_to(row, (128, 128)).T

    def mark(b, _):
        rows = pl.ds(pl.multiple_of(b * 128, 128), 128)
        first = column(ids_ref[0:1, rows].astype(f32))
        second = column(ids_ref[1:2, rows].astype(f32))
        col0[rows, :] = first
        col1[rows, :] = second
        named = (first == lanes_f) | (second == lanes_f)
        onehot[rows, :] = jnp.where(named, 1.0, 0.0).astype(bf16)
        score0 = score_ref[0:1, rows]
        score1 = score_ref[1:2, rows]
        mix0[rows, :] = column(score0 / (score0 + score1))
        mix1[rows, :] = column(score1 / (score0 + score1))
        return 0

    lax.fori_loop(0, 6, mark, 0)

    def number(b, _):
        rows = pl.ds(pl.multiple_of(b * 128, 128), 128)
        earlier = lax.broadcasted_iota(jnp.int32, (128, T), 1) < (
            lax.broadcasted_iota(jnp.int32, (128, T), 0) + b * 128
        )
        count = dot(jnp.where(earlier, 1.0, 0.0).astype(bf16), onehot[...])
        first = col0[rows, :] == lanes_f
        second = col1[rows, :] == lanes_f
        slot_t[:, rows] = jnp.where(first | second, count, -1.0).T
        place = count + base
        col0[rows, :] = jnp.broadcast_to(
            jnp.sum(jnp.where(first, place, 0.0), axis=1, keepdims=True), (128, 128)
        )
        col1[rows, :] = jnp.broadcast_to(
            jnp.sum(jnp.where(second, place, 0.0), axis=1, keepdims=True), (128, 128)
        )
        return 0

    lax.fori_loop(0, 6, number, 0)

    tok_copy.wait()

    def squares(b, _):
        rows = pl.ds(pl.multiple_of(b * 64, 64), 64)
        acc = jnp.zeros((64, 128), f32)
        for q in range(16):
            v = tok[rows, q * 128 : (q + 1) * 128].astype(f32)
            acc = acc + v * v
        rowsum[rows, :] = acc
        return 0

    lax.fori_loop(0, 12, squares, 0)

    def scale_of(b, _):
        rows = pl.ds(pl.multiple_of(b * 256, 256), 256)
        mean = jnp.sum(rowsum[rows, :], axis=1, keepdims=True) * (1.0 / D)
        rowsum[rows, :] = jnp.broadcast_to(lax.rsqrt(mean + EPS), (256, 128))
        return 0

    lax.fori_loop(0, 3, scale_of, 0)

    def normalize(b, _):
        rows = pl.ds(pl.multiple_of(b * 64, 64), 64)
        scale = rowsum[rows, :]
        for q in range(16):
            cols = slice(q * 128, (q + 1) * 128)
            v = tok[rows, cols].astype(f32) * scale * gain_ref[:, cols]
            tok[rows, cols] = v.astype(bf16)
        return 0

    lax.fori_loop(0, 12, normalize, 0)

    def pack(g, _):
        for q in range(8):
            dc, j = q // 4, q % 4
            e = source_of(g, j, dc, 1)
            first = ((x - (c + dc) % 2 + 5) % 4) // 2 * HALF
            want = lax.broadcasted_iota(jnp.int32, (HALF, T), 0) + first
            row = slot_t[pl.ds(e, 1), :]
            sel[q * HALF : (q + 1) * HALF, :] = jnp.where(
                row == want.astype(f32), 1.0, 0.0
            ).astype(bf16)
        rows = pl.ds(pl.multiple_of(g * ROWS, ROWS), ROWS)

        def part(n, _):
            cols = pl.ds(pl.multiple_of(n * 512, 512), 512)
            s_buf[rows, cols] = dot(sel[0:ROWS, :], tok[:, cols]).astype(bf16)
            return 0

        lax.fori_loop(0, 4, part, 0)
        return 0

    def dispatch(g, _):
        def one(q, _):
            k, dc, j = q // 8, (q // 4) % 2, q % 4

            @pl.when(jnp.logical_or(g < 3, q % 8 > 0))
            def _():
                row = (g * 8 + q % 8) * HALF + k * 16
                pltpu.make_async_remote_copy(
                    src_ref=at_rows(s_buf, row, 16), dst_ref=at_rows(x_buf, row, 16),
                    send_sem=s_send, recv_sem=x_recv.at[g],
                    device_id=(source_of(g, j, dc, 1), x), device_id_type=MESH,
                ).start()

            return 0

        lax.fori_loop(0, 24, one, 0)
        return 0

    def send_weight(src, dst, to, sem):
        cp = pltpu.make_async_remote_copy(
            src_ref=src, dst_ref=dst, send_sem=w_send.at[sem], recv_sem=w_recv.at[sem],
            device_id=(ep, to), device_id_type=MESH,
        )
        cp.start()
        return cp

    pack(0, 0)
    pl.semaphore_wait(barrier, 34)
    w_copies = [
        send_weight(wg_hbm, wg.at[1], x_gate, 0),
        send_weight(wu_hbm, wu.at[1], x_gate, 1),
    ]
    for k, to, parts in (
        (2, x_hid, (x_hid, x_far)), (3, x_far, (x_far, x_hid)), (1, x_gate, (x_gate, x))
    ):
        for q in range(2):
            pltpu.make_async_remote_copy(
                src_ref=wd_hbm.at[:, features(parts[q])], dst_ref=shard(k, q),
                send_sem=w_send.at[2], recv_sem=w_recv.at[2],
                device_id=(ep, to), device_id_type=MESH,
            ).start()
    dispatch(0, 0)
    for d in range(1, 4):
        pl.semaphore_signal(
            ready, inc=1, device_id=(ep, (x + d) % 4), device_id_type=MESH
        )

    def pack_and_send(g, _):
        pack(g, 0)
        dispatch(g, 0)
        return 0

    lax.fori_loop(1, 4, pack_and_send, 0)
    own = slice(24 * HALF, 25 * HALF)
    x_buf[own, :] = s_buf[own, :]

    def arrived(ref, rows, sem):
        part = ref.at[pl.ds(0, rows), :]
        pltpu.make_async_copy(part, part, sem).wait()

    wg_copy.wait()
    wu_copy.wait()
    for cp in wd_copies:
        cp.wait()
    for cp in w_copies:
        cp.wait()

    def swap(k):
        return pltpu.make_async_remote_copy(
            src_ref=h_buf.at[k], dst_ref=h_recv.at[k],
            send_sem=h_send.at[k], recv_sem=h_rsem.at[k],
            device_id=(ep, x_hid), device_id_type=MESH,
        )

    def block(k):
        return pl.ds(pl.multiple_of(k * (ROWS // 2), ROWS // 2), ROWS // 2)

    def hidden(g):
        def side(i, _):
            k = g * 2 + i
            for q in range(2):
                gate = dot(x_buf[block(k), :], wg[q])
                up = dot(x_buf[block(k), :], wu[q])
                h_buf[k, :, q * F : (q + 1) * F] = (
                    gate / (1.0 + jnp.exp(-gate)) * up
                ).astype(bf16)
            swap(k).start()
            return 0

        lax.fori_loop(0, 2, side, 0)

    def down(k):
        swap(k).wait()
        for q in range(2):
            cols = slice(q * DQ, (q + 1) * DQ)
            v = dot(h_buf[k], wd[0 : 2 * F, cols])
            v = v + dot(h_recv[k], wd[2 * F : 4 * F, cols])
            y_buf[block(k * 2 + q), :] = v.astype(bf16)

    def give(k):
        def one(n, _):
            g, side = k // 2, k % 2
            j, q = n % 4, (n // 4 + n) % 2
            src = ((k * 2 + q) * 4 + j) * HALF
            dst = ((k * 4 + j) * 2 + half) * HALF
            mine = (k == 6) & (j == 0) & (q == 0)

            @pl.when(jnp.logical_not(mine))
            def _():
                pltpu.make_async_remote_copy(
                    src_ref=at_rows(y_buf, src, HALF), dst_ref=at_rows(r_buf, dst, HALF),
                    send_sem=y_send, recv_sem=r_recv.at[g],
                    device_id=(source_of(g, j, side, -1), x + q * (x_gate - x)),
                    device_id_type=MESH,
                ).start()

            return 0

        lax.fori_loop(0, 8, one, 0)

    def expert(g, _):
        @pl.when(g < 3)
        def _():
            arrived(x_buf, ROWS, x_recv.at[g])

        @pl.when(g == 3)
        def _():
            arrived(x_buf, ROWS - HALF, x_recv.at[g])

        hidden(g)

        @pl.when(g == 2)
        def _():
            for sem in (w_send, w_recv):
                part = wd.at[pl.ds(F, 3 * F), :]
                pltpu.make_async_copy(part, part, sem.at[2]).wait()
            pl.semaphore_wait(ready, 3)

            def early(k, _):
                down(k)

                @pl.when(k < 2)
                def _():
                    give(k)

                return 0

            lax.fori_loop(0, 6, early, 0)

        @pl.when(g == 3)
        def _():
            for k in range(2, 6):
                give(k)
            for k in range(6, 8):
                down(k)
                give(k)

        return 0

    lax.fori_loop(0, 4, expert, 0)
    r_buf[pl.ds(pl.multiple_of((48 + half) * HALF, 16), HALF), :] = y_buf[
        12 * 4 * HALF : (12 * 4 + 1) * HALF, :
    ]

    comb[...] = jnp.zeros_like(comb)

    def combine(g, _):
        def weigh(b, _):
            rows = pl.ds(pl.multiple_of(b * 128, 128), 128)
            for q in range(6):
                here = (lanes + (g * 8 * CAP + q * 128)).astype(f32)
                v = jnp.where(col0[rows, :] == here, mix0[rows, :], 0.0)
                v = v + jnp.where(col1[rows, :] == here, mix1[rows, :], 0.0)
                sel[rows, q * 128 : (q + 1) * 128] = v.astype(bf16)
            return 0

        lax.fori_loop(0, 6, weigh, 0)

        @pl.when(g < 3)
        def _():
            arrived(r_buf, 16 * HALF, r_recv.at[g])

        @pl.when(g == 3)
        def _():
            arrived(r_buf, 15 * HALF, r_recv.at[g])

        rows = pl.ds(pl.multiple_of(g * 8 * CAP, 8 * CAP), 8 * CAP)
        comb[...] += dot(sel[...], r_buf[rows, :])
        return 0

    lax.fori_loop(0, 4, combine, 0)

    def square_sum(b, _):
        rows = pl.ds(pl.multiple_of(b * 128, 128), 128)
        acc = jnp.zeros((128, 128), f32)
        for q in range(4):
            v = comb[rows, q * 128 : (q + 1) * 128]
            acc = acc + v * v
        ns_buf[:, rows] = jnp.sum(acc.T.reshape(16, 8, 128), axis=0)
        return 0

    lax.fori_loop(0, 6, square_sum, 0)
    n_copies = []
    for d in range(1, 4):
        cp = pltpu.make_async_remote_copy(
            src_ref=ns_buf, dst_ref=ns_recv.at[d - 1], send_sem=n_send.at[d - 1],
            recv_sem=n_recv.at[d - 1], device_id=(ep, (x + d) % 4), device_id_type=MESH,
        )
        cp.start()
        n_copies.append(cp)
    for cp in n_copies:
        cp.wait()

    def finish(b, _):
        rows = pl.ds(pl.multiple_of(b * 128, 128), 128)
        total = ns_buf[:, rows] + ns_recv[0, :, rows] + ns_recv[1, :, rows] + ns_recv[2, :, rows]
        total = jnp.sum(total, axis=0, keepdims=True)
        scale = lax.rsqrt(total * (1.0 / D) + EPS)
        scale = jnp.broadcast_to(scale, (128, 128)).T
        for q in range(4):
            cols = slice(q * 128, (q + 1) * 128)
            out_ref[rows, cols] = (comb[rows, cols] * scale * og_ref[:, cols]).astype(bf16)
        return 0

    lax.fori_loop(0, 6, finish, 0)

    arrived(s_buf, 31 * HALF, s_send)

    arrived(y_buf, 63 * HALF, y_send)


def per_device(
    tokens, in_gain, route_ids, route_scores, gate_weight, up_weight, down_weight, out_gain
):
    vmem = pl.BlockSpec(memory_space=pltpu.VMEM)
    hbm = pl.BlockSpec(memory_space=pl.ANY)
    dma = pltpu.SemaphoreType.DMA
    return pl.pallas_call(
        kernel,
        out_shape=jax.ShapeDtypeStruct((T, DQ), bf16),
        in_specs=[hbm, vmem, vmem, vmem, hbm, hbm, hbm, vmem],
        out_specs=vmem,
        scratch_shapes=[
            pltpu.VMEM((T, D), bf16),
            pltpu.VMEM((4 * ROWS, D), bf16),
            pltpu.VMEM((4 * ROWS, D), bf16),
            pltpu.VMEM((2, D, F), bf16),
            pltpu.VMEM((2, D, F), bf16),
            pltpu.VMEM((4 * F, 2 * DQ), bf16),
            pltpu.VMEM((8, ROWS // 2, 2 * F), bf16),
            pltpu.VMEM((8, ROWS // 2, 2 * F), bf16),
            pltpu.VMEM((64 * HALF, DQ), bf16),
            pltpu.VMEM((64 * HALF, DQ), bf16),
            pltpu.VMEM((128, T), f32),
            pltpu.VMEM((T, 128), bf16),
            pltpu.VMEM((T, T), bf16),
            pltpu.VMEM((T, 128), f32),
            pltpu.VMEM((T, 128), f32),
            pltpu.VMEM((T, 128), f32),
            pltpu.VMEM((T, 128), f32),
            pltpu.VMEM((T, 128), f32),
            pltpu.VMEM((T, DQ), f32),
            pltpu.VMEM((8, T), f32),
            pltpu.VMEM((3, 8, T), f32),
            dma((5,)),
            dma,
            dma((4,)),
            dma((3,)),
            dma((3,)),
            dma((8,)),
            dma((8,)),
            dma,
            dma((4,)),
            dma((3,)),
            dma((3,)),
            pltpu.SemaphoreType.REGULAR,
        ],
        compiler_params=pltpu.CompilerParams(
            collective_id=0, has_side_effects=True, vmem_limit_bytes=62 * 2**20
        ),
        name="routed_experts",
    )(
        tokens,
        in_gain.reshape(1, D),
        route_ids.T,
        route_scores.T,
        gate_weight.reshape(D, F),
        up_weight.reshape(D, F),
        down_weight.reshape(F, D),
        out_gain.reshape(1, DQ),
    )


def solution(mesh):
    in_specs = (
        P("ep", None),
        P(),
        P("ep", None),
        P("ep", None),
        P("ep", None, "tp"),
        P("ep", None, "tp"),
        P("ep", "tp", None),
        P("tp"),
    )
    return jax.shard_map(
        per_device, mesh=mesh, in_specs=in_specs, out_specs=P("ep", "tp"), check_vma=False
    )
```

```python
import jax
import jax.numpy as jnp
from jax import lax
from jax.experimental import pallas as pl
from jax.experimental.pallas import tpu as pltpu
from jax.sharding import PartitionSpec as P

EPS = 1e-06
MESH = pl.DeviceIdType.MESH
T = 768
D = 2048
F = 256
CAP = 96
HALF = 48
ROWS = 4 * 2 * HALF
DQ = 512
STEPS = (
    (2, 2), (1, 2), (2, 1), (3, 2),
    (2, 3), (1, 1), (1, 3), (3, 1),
    (3, 3), (2, 0), (0, 2), (0, 1),
    (1, 0), (0, 3), (3, 0), (0, 0),
)
FAR = 5
OWN = 3 * 8 + 3
f32 = jnp.float32
bf16 = jnp.bfloat16


def dot(a, b):
    return jnp.dot(a, b, preferred_element_type=f32)


def at_rows(ref, start, size):
    return ref.at[pl.ds(pl.multiple_of(start, 16), size), :]


def kernel(
    tok_hbm, gain_ref, ids_ref, score_ref, wg_hbm, wu_hbm, wd_hbm, og_ref,
    out_ref,
    tok, s_buf, x_buf, wg, wu, wd, h_buf, h_recv, y_buf, r_buf,
    slot_t, onehot, sel, col0, col1, mix0, mix1, rowsum, comb, ns_buf, ns_recv,
    local_sem, s_send, x_recv, f_send, f_recv, w_send, w_recv, h_send, h_rsem, y_send, r_recv, n_send, n_recv, ready,
):
    ep = lax.axis_index("ep")
    x = lax.axis_index("tp")
    z = ep // 8
    y = (ep // 2) % 4
    c = ep % 2
    xs = (x - c + 5) % 4
    half = xs // 2
    member = xs % 2
    x_gate = ((((x - c + 4) % 4) + 1 - 2 * (((x - c + 4) % 4) % 2)) + c) % 4
    x_hid = (xs + 1 - 2 * member + c + 3) % 4
    x_far = (x + 2) % 4

    def peer(p, dc, sign):
        dz, dy = STEPS[p]
        return (
            ((z + sign * dz + 4) % 4) * 8 + ((y + sign * dy + 4) % 4) * 2 + (c + dc) % 2
        )

    tok_copy = pltpu.make_async_copy(tok_hbm, tok, local_sem.at[0])
    tok_copy.start()
    wg_copy = pltpu.make_async_copy(wg_hbm, wg.at[0], local_sem.at[1])
    wu_copy = pltpu.make_async_copy(wu_hbm, wu.at[0], local_sem.at[2])

    def features(k):
        return pl.ds(pl.multiple_of(k * DQ, DQ), DQ)

    def shard(k, part):
        return wd.at[pl.ds(k * F, F), pl.ds(part * DQ, DQ)]

    wd_copies = [
        pltpu.make_async_copy(wd_hbm.at[:, features(k)], shard(0, q), local_sem.at[3 + q])
        for q, k in enumerate((x, x_gate))
    ]
    wg_copy.start()
    wu_copy.start()
    for cp in wd_copies:
        cp.start()

    barrier = pltpu.get_barrier_semaphore()

    def greet(i, _):
        pl.semaphore_signal(
            barrier, inc=1, device_id=((ep + i) % 32, x), device_id_type=MESH
        )
        return 0

    lax.fori_loop(1, 32, greet, 0)
    for d in range(1, 4):
        pl.semaphore_signal(
            barrier, inc=1, device_id=(ep, (x + d) % 4), device_id_type=MESH
        )

    lanes = lax.broadcasted_iota(jnp.int32, (128, 128), 1)
    dz_l = ((lanes >> 3) - z) & 3
    dy_l = (((lanes >> 1) & 3) - y) & 3
    dc_l = ((lanes & 1) - c) & 1
    base = dc_l * (4 * CAP)
    for p, (dz, dy) in enumerate(STEPS):
        base = base + jnp.where(
            dz_l * 4 + dy_l == dz * 4 + dy, (p // 4 * 8 + p % 4) * CAP, 0
        )
    base = base.astype(f32)
    lanes_f = lanes.astype(f32)

    def column(row):
        return jnp.broadcast_to(row, (128, 128)).T

    def mark(b, _):
        rows = pl.ds(pl.multiple_of(b * 128, 128), 128)
        first = column(ids_ref[0:1, rows].astype(f32))
        second = column(ids_ref[1:2, rows].astype(f32))
        col0[rows, :] = first
        col1[rows, :] = second
        named = (first == lanes_f) | (second == lanes_f)
        onehot[rows, :] = jnp.where(named, 1.0, 0.0).astype(bf16)
        score0 = score_ref[0:1, rows]
        score1 = score_ref[1:2, rows]
        mix0[rows, :] = column(score0 / (score0 + score1))
        mix1[rows, :] = column(score1 / (score0 + score1))
        return 0

    lax.fori_loop(0, 6, mark, 0)

    def number(b, _):
        rows = pl.ds(pl.multiple_of(b * 128, 128), 128)
        earlier = lax.broadcasted_iota(jnp.int32, (128, T), 1) < (
            lax.broadcasted_iota(jnp.int32, (128, T), 0) + b * 128
        )
        count = dot(jnp.where(earlier, 1.0, 0.0).astype(bf16), onehot[...])
        first = col0[rows, :] == lanes_f
        second = col1[rows, :] == lanes_f
        slot_t[:, rows] = jnp.where(first | second, count, -1.0).T
        place = count + base
        col0[rows, :] = jnp.broadcast_to(
            jnp.sum(jnp.where(first, place, 0.0), axis=1, keepdims=True), (128, 128)
        )
        col1[rows, :] = jnp.broadcast_to(
            jnp.sum(jnp.where(second, place, 0.0), axis=1, keepdims=True), (128, 128)
        )
        return 0

    lax.fori_loop(0, 6, number, 0)

    tok_copy.wait()

    def squares(b, _):
        rows = pl.ds(pl.multiple_of(b * 64, 64), 64)
        acc = jnp.zeros((64, 128), f32)
        for q in range(16):
            v = tok[rows, q * 128 : (q + 1) * 128].astype(f32)
            acc = acc + v * v
        rowsum[rows, :] = acc
        return 0

    lax.fori_loop(0, 12, squares, 0)

    def scale_of(b, _):
        rows = pl.ds(pl.multiple_of(b * 256, 256), 256)
        mean = jnp.sum(rowsum[rows, :], axis=1, keepdims=True) * (1.0 / D)
        rowsum[rows, :] = jnp.broadcast_to(lax.rsqrt(mean + EPS), (256, 128))
        return 0

    lax.fori_loop(0, 3, scale_of, 0)

    def normalize(b, _):
        rows = pl.ds(pl.multiple_of(b * 64, 64), 64)
        scale = rowsum[rows, :]
        for q in range(16):
            cols = slice(q * 128, (q + 1) * 128)
            v = tok[rows, cols].astype(f32) * scale * gain_ref[:, cols]
            tok[rows, cols] = v.astype(bf16)
        return 0

    lax.fori_loop(0, 12, normalize, 0)

    def pack(g):
        for q in range(8):
            dc, j = q // 4, q % 4
            e = peer(g * 4 + j, dc, 1)
            first = ((x - (c + dc) % 2 + 5) % 4) // 2 * HALF
            want = lax.broadcasted_iota(jnp.int32, (HALF, T), 0) + first
            row = slot_t[pl.ds(e, 1), :]
            sel[q * HALF : (q + 1) * HALF, :] = jnp.where(
                row == want.astype(f32), 1.0, 0.0
            ).astype(bf16)
        rows = slice(g * ROWS, (g + 1) * ROWS)

        def part(n, _):
            cols = pl.ds(pl.multiple_of(n * 512, 512), 512)
            s_buf[rows, cols] = dot(sel[0:ROWS, :], tok[:, cols]).astype(bf16)
            return 0

        lax.fori_loop(0, 4, part, 0)

    far_parity = (x + c + 1) % 2

    def dispatch(steps, sem):
        def one(n, _):
            k, dc = n // 2, n % 2
            for p in steps:
                if p == 15:
                    go = dc > 0
                elif p < FAR:
                    go = far_parity == p % 2
                else:
                    go = dc >= 0

                @pl.when(go)
                def _():
                    row = (p // 4 * 8 + dc * 4 + p % 4) * HALF + k * 16
                    pltpu.make_async_remote_copy(
                        src_ref=at_rows(s_buf, row, 16), dst_ref=at_rows(x_buf, row, 16),
                        send_sem=s_send, recv_sem=x_recv.at[sem],
                        device_id=(peer(p, dc, 1), x), device_id_type=MESH,
                    ).start()

            return 0

        lax.fori_loop(0, 6, one, 0)

    def send_weight(src, dst, to, sem):
        cp = pltpu.make_async_remote_copy(
            src_ref=src, dst_ref=dst, send_sem=w_send.at[sem], recv_sem=w_recv.at[sem],
            device_id=(ep, to), device_id_type=MESH,
        )
        cp.start()
        return cp

    pack(0)
    pl.semaphore_wait(barrier, 34)
    w_copies = [
        send_weight(wg_hbm, wg.at[1], x_gate, 0),
        send_weight(wu_hbm, wu.at[1], x_gate, 1),
    ]
    for k, to, parts in (
        (2, x_hid, (x_hid, x_far)), (3, x_far, (x_far, x_hid)), (1, x_gate, (x_gate, x))
    ):
        for q in range(2):
            pltpu.make_async_remote_copy(
                src_ref=wd_hbm.at[:, features(parts[q])], dst_ref=shard(k, q),
                send_sem=w_send.at[2], recv_sem=w_recv.at[2],
                device_id=(ep, to), device_id_type=MESH,
            ).start()
    dispatch(range(4), 0)
    for d in range(1, 4):
        pl.semaphore_signal(
            ready, inc=1, device_id=(ep, (x + d) % 4), device_id_type=MESH
        )
    pack(1)
    dispatch(range(4, FAR), 0)
    dispatch(range(FAR, 8), 1)
    pack(2)
    dispatch(range(8, 12), 2)
    pack(3)
    dispatch(range(12, 16), 3)
    own = slice(OWN * HALF, (OWN + 1) * HALF)
    x_buf[own, :] = s_buf[own, :]

    def arrived(ref, rows, sem):
        part = ref.at[pl.ds(0, rows), :]
        pltpu.make_async_copy(part, part, sem).wait()

    def hand(p):
        row = (p // 4 * 8 + (member + p) % 2 * 4 + p % 4) * HALF
        return pltpu.make_async_remote_copy(
            src_ref=at_rows(x_buf, row, HALF), dst_ref=at_rows(x_buf, row, HALF),
            send_sem=f_send, recv_sem=f_recv,
            device_id=(ep, x_hid), device_id_type=MESH,
        )

    arrived(x_buf, FAR * HALF, x_recv.at[0])
    for p in range(FAR):
        hand(p).start()

    wg_copy.wait()
    wu_copy.wait()
    for cp in wd_copies:
        cp.wait()
    for cp in w_copies:
        cp.wait()

    def swap(k):
        return pltpu.make_async_remote_copy(
            src_ref=h_buf.at[k], dst_ref=h_recv.at[k],
            send_sem=h_send.at[k], recv_sem=h_rsem.at[k],
            device_id=(ep, x_hid), device_id_type=MESH,
        )

    def block(k):
        return pl.ds(pl.multiple_of(k * (ROWS // 2), ROWS // 2), ROWS // 2)

    def hidden(g):
        def side(i, _):
            k = g * 2 + i
            for q in range(2):
                gate = dot(x_buf[block(k), :], wg[q])
                up = dot(x_buf[block(k), :], wu[q])
                h_buf[k, :, q * F : (q + 1) * F] = (
                    gate / (1.0 + jnp.exp(-gate)) * up
                ).astype(bf16)
            swap(k).start()
            return 0

        lax.fori_loop(0, 2, side, 0)

    def down(k):
        swap(k).wait()
        for q in range(2):
            cols = slice(q * DQ, (q + 1) * DQ)
            v = dot(h_buf[k], wd[0 : 2 * F, cols])
            v = v + dot(h_recv[k], wd[2 * F : 4 * F, cols])
            y_buf[block(k * 2 + q), :] = v.astype(bf16)

    def give(g, side):
        k = g * 2 + side
        for n in range(8):
            j, q = n % 4, (n // 4 + n) % 2
            src = ((k * 2 + q) * 4 + j) * HALF
            dst = ((k * 4 + j) * 2 + half) * HALF

            def one():
                pltpu.make_async_remote_copy(
                    src_ref=at_rows(y_buf, src, HALF), dst_ref=at_rows(r_buf, dst, HALF),
                    send_sem=y_send, recv_sem=r_recv.at[g],
                    device_id=(peer(g * 4 + j, side, -1), (x, x_gate)[q]),
                    device_id_type=MESH,
                ).start()

            if (g, j, q) == (3, 3, 0):
                pl.when(side > 0)(one)
            else:
                one()

    def finish_group(g):
        def one(side, _):
            down(g * 2 + side)
            give(g, side)
            return 0

        lax.fori_loop(0, 2, one, 0)

    arrived(x_buf, (8 - FAR) * 2 * HALF, x_recv.at[1])
    for sem in (f_send, f_recv):
        arrived(x_buf, FAR * HALF, sem)
    hidden(1)
    hidden(0)
    for sem in (w_send, w_recv):
        part = wd.at[pl.ds(F, 3 * F), :]
        pltpu.make_async_copy(part, part, sem.at[2]).wait()
    pl.semaphore_wait(ready, 3)
    finish_group(1)
    arrived(x_buf, ROWS, x_recv.at[2])
    hidden(2)
    finish_group(0)
    arrived(x_buf, ROWS - HALF, x_recv.at[3])
    hidden(3)
    finish_group(2)
    finish_group(3)
    r_buf[pl.ds(pl.multiple_of((OWN * 2 + half) * HALF, 16), HALF), :] = y_buf[
        (12 * 4 + 3) * HALF : (12 * 4 + 4) * HALF, :
    ]

    comb[...] = jnp.zeros_like(comb)

    def combine(i, _):
        g = i + (1 - 2 * (i % 2)) * (1 - i // 2)

        def weigh(b, _):
            rows = pl.ds(pl.multiple_of(b * 128, 128), 128)
            for q in range(6):
                here = (lanes + (g * 8 * CAP + q * 128)).astype(f32)
                v = jnp.where(col0[rows, :] == here, mix0[rows, :], 0.0)
                v = v + jnp.where(col1[rows, :] == here, mix1[rows, :], 0.0)
                sel[rows, q * 128 : (q + 1) * 128] = v.astype(bf16)
            return 0

        lax.fori_loop(0, 6, weigh, 0)

        @pl.when(g < 3)
        def _():
            arrived(r_buf, 16 * HALF, r_recv.at[g])

        @pl.when(g == 3)
        def _():
            arrived(r_buf, 15 * HALF, r_recv.at[g])

        rows = pl.ds(pl.multiple_of(g * 8 * CAP, 8 * CAP), 8 * CAP)
        comb[...] += dot(sel[...], r_buf[rows, :])
        return 0

    lax.fori_loop(0, 4, combine, 0)

    def square_sum(b, _):
        rows = pl.ds(pl.multiple_of(b * 128, 128), 128)
        acc = jnp.zeros((128, 128), f32)
        for q in range(4):
            v = comb[rows, q * 128 : (q + 1) * 128]
            acc = acc + v * v
        ns_buf[:, rows] = jnp.sum(acc.T.reshape(16, 8, 128), axis=0)
        return 0

    lax.fori_loop(0, 6, square_sum, 0)
    n_copies = []
    for d in range(1, 4):
        cp = pltpu.make_async_remote_copy(
            src_ref=ns_buf, dst_ref=ns_recv.at[d - 1], send_sem=n_send.at[d - 1],
            recv_sem=n_recv.at[d - 1], device_id=(ep, (x + d) % 4), device_id_type=MESH,
        )
        cp.start()
        n_copies.append(cp)
    for cp in n_copies:
        cp.wait()

    def finish(b, _):
        rows = pl.ds(pl.multiple_of(b * 128, 128), 128)
        total = ns_buf[:, rows] + ns_recv[0, :, rows] + ns_recv[1, :, rows] + ns_recv[2, :, rows]
        total = jnp.sum(total, axis=0, keepdims=True)
        scale = lax.rsqrt(total * (1.0 / D) + EPS)
        scale = jnp.broadcast_to(scale, (128, 128)).T
        for q in range(4):
            cols = slice(q * 128, (q + 1) * 128)
            out_ref[rows, cols] = (comb[rows, cols] * scale * og_ref[:, cols]).astype(bf16)
        return 0

    lax.fori_loop(0, 6, finish, 0)

    @pl.when(far_parity == 0)
    def _():
        arrived(s_buf, 27 * HALF, s_send)

    @pl.when(far_parity == 1)
    def _():
        arrived(s_buf, 25 * HALF, s_send)


    arrived(y_buf, 63 * HALF, y_send)


def per_device(
    tokens, in_gain, route_ids, route_scores, gate_weight, up_weight, down_weight, out_gain
):
    vmem = pl.BlockSpec(memory_space=pltpu.VMEM)
    hbm = pl.BlockSpec(memory_space=pl.ANY)
    dma = pltpu.SemaphoreType.DMA
    return pl.pallas_call(
        kernel,
        out_shape=jax.ShapeDtypeStruct((T, DQ), bf16),
        in_specs=[hbm, vmem, vmem, vmem, hbm, hbm, hbm, vmem],
        out_specs=vmem,
        scratch_shapes=[
            pltpu.VMEM((T, D), bf16),
            pltpu.VMEM((4 * ROWS, D), bf16),
            pltpu.VMEM((4 * ROWS, D), bf16),
            pltpu.VMEM((2, D, F), bf16),
            pltpu.VMEM((2, D, F), bf16),
            pltpu.VMEM((4 * F, 2 * DQ), bf16),
            pltpu.VMEM((8, ROWS // 2, 2 * F), bf16),
            pltpu.VMEM((8, ROWS // 2, 2 * F), bf16),
            pltpu.VMEM((64 * HALF, DQ), bf16),
            pltpu.VMEM((64 * HALF, DQ), bf16),
            pltpu.VMEM((128, T), f32),
            pltpu.VMEM((T, 128), bf16),
            pltpu.VMEM((T, T), bf16),
            pltpu.VMEM((T, 128), f32),
            pltpu.VMEM((T, 128), f32),
            pltpu.VMEM((T, 128), f32),
            pltpu.VMEM((T, 128), f32),
            pltpu.VMEM((T, 128), f32),
            pltpu.VMEM((T, DQ), f32),
            pltpu.VMEM((8, T), f32),
            pltpu.VMEM((3, 8, T), f32),
            dma((5,)),
            dma,
            dma((4,)),
            dma,
            dma,
            dma((3,)),
            dma((3,)),
            dma((8,)),
            dma((8,)),
            dma,
            dma((4,)),
            dma((3,)),
            dma((3,)),
            pltpu.SemaphoreType.REGULAR,
        ],
        compiler_params=pltpu.CompilerParams(
            collective_id=0, has_side_effects=True, vmem_limit_bytes=62 * 2**20
        ),
        name="routed_experts",
    )(
        tokens,
        in_gain.reshape(1, D),
        route_ids.T,
        route_scores.T,
        gate_weight.reshape(D, F),
        up_weight.reshape(D, F),
        down_weight.reshape(F, D),
        out_gain.reshape(1, DQ),
    )


def solution(mesh):
    in_specs = (
        P("ep", None),
        P(),
        P("ep", None),
        P("ep", None),
        P("ep", None, "tp"),
        P("ep", None, "tp"),
        P("ep", "tp", None),
        P("tp"),
    )
    return jax.shard_map(
        per_device, mesh=mesh, in_specs=in_specs, out_specs=P("ep", "tp"), check_vma=False
    )
```

```python
import jax
import jax.numpy as jnp
from jax import lax
from jax.experimental import pallas as pl
from jax.experimental.pallas import tpu as pltpu
from jax.sharding import PartitionSpec as P

EPS = 1e-06
MESH = pl.DeviceIdType.MESH
T = 768
D = 2048
F = 256
CAP = 96
HALF = 48
ROWS = 4 * 2 * HALF
DQ = 512
STEPS = (
    (2, 2), (1, 2), (2, 3), (2, 1),
    (3, 2), (0, 1), (0, 3), (2, 0),
    (1, 1), (3, 3), (0, 2), (1, 0),
    (1, 3), (3, 1), (3, 0), (0, 0),
)
FAR = 5
OWN = 3 * 8 + 3
f32 = jnp.float32
bf16 = jnp.bfloat16


def dot(a, b):
    return jnp.dot(a, b, preferred_element_type=f32)


def at_rows(ref, start, size):
    return ref.at[pl.ds(pl.multiple_of(start, 16), size), :]


def kernel(
    tok_hbm, gain_ref, ids_ref, score_ref, wg_hbm, wu_hbm, wd_hbm, og_ref,
    out_ref,
    tok, s_buf, x_buf, wg, wu, wd, h_buf, h_recv, y_buf, r_buf,
    slot_t, onehot, sel, col0, col1, mix0, mix1, rowsum, comb, ns_buf, ns_recv,
    local_sem, s_send, x_recv, f_send, f_recv, w_send, w_recv, h_send, h_rsem, y_send, r_recv, n_send, n_recv, ready,
):
    ep = lax.axis_index("ep")
    x = lax.axis_index("tp")
    z = ep // 8
    y = (ep // 2) % 4
    c = ep % 2
    xs = (x - c + 5) % 4
    half = xs // 2
    member = xs % 2
    x_gate = ((((x - c + 4) % 4) + 1 - 2 * (((x - c + 4) % 4) % 2)) + c) % 4
    x_hid = (xs + 1 - 2 * member + c + 3) % 4
    x_far = (x + 2) % 4

    def peer(p, dc, sign):
        dz, dy = STEPS[p]
        return (
            ((z + sign * dz + 4) % 4) * 8 + ((y + sign * dy + 4) % 4) * 2 + (c + dc) % 2
        )

    tok_copy = pltpu.make_async_copy(tok_hbm, tok, local_sem.at[0])
    tok_copy.start()
    wg_copy = pltpu.make_async_copy(wg_hbm, wg.at[0], local_sem.at[1])
    wu_copy = pltpu.make_async_copy(wu_hbm, wu.at[0], local_sem.at[2])

    def features(k):
        return pl.ds(pl.multiple_of(k * DQ, DQ), DQ)

    def shard(k, part):
        return wd.at[pl.ds(k * F, F), pl.ds(part * DQ, DQ)]

    wd_copies = [
        pltpu.make_async_copy(wd_hbm.at[:, features(k)], shard(0, q), local_sem.at[3 + q])
        for q, k in enumerate((x, x_gate))
    ]
    wg_copy.start()
    wu_copy.start()
    for cp in wd_copies:
        cp.start()

    barrier = pltpu.get_barrier_semaphore()

    def greet(i, _):
        pl.semaphore_signal(
            barrier, inc=1, device_id=((ep + i) % 32, x), device_id_type=MESH
        )
        return 0

    lax.fori_loop(1, 32, greet, 0)
    for d in range(1, 4):
        pl.semaphore_signal(
            barrier, inc=1, device_id=(ep, (x + d) % 4), device_id_type=MESH
        )

    lanes = lax.broadcasted_iota(jnp.int32, (128, 128), 1)
    dz_l = ((lanes >> 3) - z) & 3
    dy_l = (((lanes >> 1) & 3) - y) & 3
    dc_l = ((lanes & 1) - c) & 1
    base = dc_l * (4 * CAP)
    for p, (dz, dy) in enumerate(STEPS):
        base = base + jnp.where(
            dz_l * 4 + dy_l == dz * 4 + dy, (p // 4 * 8 + p % 4) * CAP, 0
        )
    base = base.astype(f32)
    lanes_f = lanes.astype(f32)

    def column(row):
        return jnp.broadcast_to(row, (128, 128)).T

    def mark(b, _):
        rows = pl.ds(pl.multiple_of(b * 128, 128), 128)
        first = column(ids_ref[0:1, rows].astype(f32))
        second = column(ids_ref[1:2, rows].astype(f32))
        col0[rows, :] = first
        col1[rows, :] = second
        named = (first == lanes_f) | (second == lanes_f)
        onehot[rows, :] = jnp.where(named, 1.0, 0.0).astype(bf16)
        score0 = score_ref[0:1, rows]
        score1 = score_ref[1:2, rows]
        mix0[rows, :] = column(score0 / (score0 + score1))
        mix1[rows, :] = column(score1 / (score0 + score1))
        return 0

    lax.fori_loop(0, 6, mark, 0)

    def number(b, _):
        rows = pl.ds(pl.multiple_of(b * 128, 128), 128)
        earlier = lax.broadcasted_iota(jnp.int32, (128, T), 1) < (
            lax.broadcasted_iota(jnp.int32, (128, T), 0) + b * 128
        )
        count = dot(jnp.where(earlier, 1.0, 0.0).astype(bf16), onehot[...])
        first = col0[rows, :] == lanes_f
        second = col1[rows, :] == lanes_f
        slot_t[:, rows] = jnp.where(first | second, count, -1.0).T
        place = count + base
        col0[rows, :] = jnp.broadcast_to(
            jnp.sum(jnp.where(first, place, 0.0), axis=1, keepdims=True), (128, 128)
        )
        col1[rows, :] = jnp.broadcast_to(
            jnp.sum(jnp.where(second, place, 0.0), axis=1, keepdims=True), (128, 128)
        )
        return 0

    lax.fori_loop(0, 6, number, 0)

    tok_copy.wait()

    def squares(b, _):
        rows = pl.ds(pl.multiple_of(b * 64, 64), 64)
        acc = jnp.zeros((64, 128), f32)
        for q in range(16):
            v = tok[rows, q * 128 : (q + 1) * 128].astype(f32)
            acc = acc + v * v
        rowsum[rows, :] = acc
        return 0

    lax.fori_loop(0, 12, squares, 0)

    def scale_of(b, _):
        rows = pl.ds(pl.multiple_of(b * 256, 256), 256)
        mean = jnp.sum(rowsum[rows, :], axis=1, keepdims=True) * (1.0 / D)
        rowsum[rows, :] = jnp.broadcast_to(lax.rsqrt(mean + EPS), (256, 128))
        return 0

    lax.fori_loop(0, 3, scale_of, 0)

    def normalize(b, _):
        rows = pl.ds(pl.multiple_of(b * 64, 64), 64)
        scale = rowsum[rows, :]
        for q in range(16):
            cols = slice(q * 128, (q + 1) * 128)
            v = tok[rows, cols].astype(f32) * scale * gain_ref[:, cols]
            tok[rows, cols] = v.astype(bf16)
        return 0

    lax.fori_loop(0, 12, normalize, 0)

    def pack(g):
        for q in range(8):
            dc, j = q // 4, q % 4
            e = peer(g * 4 + j, dc, 1)
            first = ((x - (c + dc) % 2 + 5) % 4) // 2 * HALF
            want = lax.broadcasted_iota(jnp.int32, (HALF, T), 0) + first
            row = slot_t[pl.ds(e, 1), :]
            sel[q * HALF : (q + 1) * HALF, :] = jnp.where(
                row == want.astype(f32), 1.0, 0.0
            ).astype(bf16)
        rows = slice(g * ROWS, (g + 1) * ROWS)

        def part(n, _):
            cols = pl.ds(pl.multiple_of(n * 512, 512), 512)
            s_buf[rows, cols] = dot(sel[0:ROWS, :], tok[:, cols]).astype(bf16)
            return 0

        lax.fori_loop(0, 4, part, 0)

    far_parity = (x + c + 1) % 2

    def dispatch(steps):
        def one(n, _):
            k, dc = n // 2, n % 2
            for p in steps:
                if p == 15:
                    go = dc > 0
                elif p < FAR:
                    go = far_parity == p % 2
                else:
                    go = dc >= 0

                @pl.when(go)
                def _():
                    row = (p // 4 * 8 + dc * 4 + p % 4) * HALF + k * 16
                    pltpu.make_async_remote_copy(
                        src_ref=at_rows(s_buf, row, 16), dst_ref=at_rows(x_buf, row, 16),
                        send_sem=s_send, recv_sem=x_recv.at[0 if p < FAR else p // 4],
                        device_id=(peer(p, dc, 1), x), device_id_type=MESH,
                    ).start()

            return 0

        lax.fori_loop(0, 6, one, 0)

    def send_weight(src, dst, to, sem):
        cp = pltpu.make_async_remote_copy(
            src_ref=src, dst_ref=dst, send_sem=w_send.at[sem], recv_sem=w_recv.at[sem],
            device_id=(ep, to), device_id_type=MESH,
        )
        cp.start()
        return cp

    pack(0)
    pl.semaphore_wait(barrier, 34)
    w_copies = [
        send_weight(wg_hbm, wg.at[1], x_gate, 0),
        send_weight(wu_hbm, wu.at[1], x_gate, 1),
    ]
    for k, to, parts in ((2, x_hid, (x_hid, x_far)), (1, x_gate, (x_gate, x))):
        for q in range(2):
            pltpu.make_async_remote_copy(
                src_ref=wd_hbm.at[:, features(parts[q])], dst_ref=shard(k, q),
                send_sem=w_send.at[1 + k], recv_sem=w_recv.at[1 + k],
                device_id=(ep, to), device_id_type=MESH,
            ).start()
    dispatch(range(4))
    for d in range(1, 4):
        pl.semaphore_signal(
            ready, inc=1, device_id=(ep, (x + d) % 4), device_id_type=MESH
        )
    pack(1)
    dispatch(range(4, 8))
    pack(2)
    dispatch(range(8, 12))
    pack(3)
    dispatch(range(12, 16))
    own = slice(OWN * HALF, (OWN + 1) * HALF)
    x_buf[own, :] = s_buf[own, :]

    def arrived(ref, rows, sem):
        part = ref.at[pl.ds(0, rows), :]
        pltpu.make_async_copy(part, part, sem).wait()

    def shard_copied(k):
        part = wd.at[pl.ds(k * F, F), :]
        for sem in (w_send, w_recv):
            pltpu.make_async_copy(part, part, sem.at[1 + k]).wait()

    def relay():
        shard_copied(2)
        for q in range(2):
            pltpu.make_async_remote_copy(
                src_ref=shard(2, 1 - q), dst_ref=shard(3, q),
                send_sem=w_send.at[4], recv_sem=w_recv.at[4],
                device_id=(ep, x_gate), device_id_type=MESH,
            ).start()

    def hand(p):
        row = (p // 4 * 8 + (member + p) % 2 * 4 + p % 4) * HALF
        return pltpu.make_async_remote_copy(
            src_ref=at_rows(x_buf, row, HALF), dst_ref=at_rows(x_buf, row, HALF),
            send_sem=f_send, recv_sem=f_recv,
            device_id=(ep, x_hid), device_id_type=MESH,
        )

    arrived(x_buf, FAR * HALF, x_recv.at[0])
    for p in range(FAR):
        hand(p).start()

    wg_copy.wait()
    wu_copy.wait()
    for cp in wd_copies:
        cp.wait()
    for cp in w_copies:
        cp.wait()
    relay()

    def swap(k):
        return pltpu.make_async_remote_copy(
            src_ref=h_buf.at[k], dst_ref=h_recv.at[k],
            send_sem=h_send.at[k], recv_sem=h_rsem.at[k],
            device_id=(ep, x_hid), device_id_type=MESH,
        )

    def block(k):
        return pl.ds(pl.multiple_of(k * (ROWS // 2), ROWS // 2), ROWS // 2)

    def hidden(g):
        def side(i, _):
            k = g * 2 + i
            for q in range(2):
                gate = dot(x_buf[block(k), :], wg[q])
                up = dot(x_buf[block(k), :], wu[q])
                h_buf[k, :, q * F : (q + 1) * F] = (
                    gate / (1.0 + jnp.exp(-gate)) * up
                ).astype(bf16)
            swap(k).start()
            return 0

        lax.fori_loop(0, 2, side, 0)

    def down(k):
        swap(k).wait()
        for q in range(2):
            cols = slice(q * DQ, (q + 1) * DQ)
            v = dot(h_buf[k], wd[0 : 2 * F, cols])
            v = v + dot(h_recv[k], wd[2 * F : 4 * F, cols])
            y_buf[block(k * 2 + q), :] = v.astype(bf16)

    def give(g, side):
        k = g * 2 + side
        for n in range(8):
            j, q = n % 4, (n // 4 + n) % 2
            src = ((k * 2 + q) * 4 + j) * HALF
            dst = ((k * 4 + j) * 2 + half) * HALF

            def one():
                pltpu.make_async_remote_copy(
                    src_ref=at_rows(y_buf, src, HALF), dst_ref=at_rows(r_buf, dst, HALF),
                    send_sem=y_send, recv_sem=r_recv.at[g],
                    device_id=(peer(g * 4 + j, side, -1), (x, x_gate)[q]),
                    device_id_type=MESH,
                ).start()

            if (g, j, q) == (3, 3, 0):
                pl.when(side > 0)(one)
            else:
                one()

    def finish_group(g):
        def one(side, _):
            down(g * 2 + side)
            give(g, side)
            return 0

        lax.fori_loop(0, 2, one, 0)

    arrived(x_buf, (8 - FAR) * 2 * HALF, x_recv.at[1])
    for sem in (f_send, f_recv):
        arrived(x_buf, FAR * HALF, sem)
    hidden(1)
    hidden(0)
    shard_copied(1)
    shard_copied(3)
    pl.semaphore_wait(ready, 3)
    finish_group(1)
    arrived(x_buf, ROWS, x_recv.at[2])
    hidden(2)
    finish_group(0)
    arrived(x_buf, ROWS - HALF, x_recv.at[3])
    hidden(3)
    finish_group(2)
    finish_group(3)
    r_buf[pl.ds(pl.multiple_of((OWN * 2 + half) * HALF, 16), HALF), :] = y_buf[
        (12 * 4 + 3) * HALF : (12 * 4 + 4) * HALF, :
    ]

    comb[...] = jnp.zeros_like(comb)

    def combine(i, _):
        g = i + (1 - 2 * (i % 2)) * (1 - i // 2)

        def weigh(b, _):
            rows = pl.ds(pl.multiple_of(b * 128, 128), 128)
            for q in range(6):
                here = (lanes + (g * 8 * CAP + q * 128)).astype(f32)
                v = jnp.where(col0[rows, :] == here, mix0[rows, :], 0.0)
                v = v + jnp.where(col1[rows, :] == here, mix1[rows, :], 0.0)
                sel[rows, q * 128 : (q + 1) * 128] = v.astype(bf16)
            return 0

        lax.fori_loop(0, 6, weigh, 0)

        @pl.when(g < 3)
        def _():
            arrived(r_buf, 16 * HALF, r_recv.at[g])

        @pl.when(g == 3)
        def _():
            arrived(r_buf, 15 * HALF, r_recv.at[g])

        rows = pl.ds(pl.multiple_of(g * 8 * CAP, 8 * CAP), 8 * CAP)
        comb[...] += dot(sel[...], r_buf[rows, :])
        return 0

    lax.fori_loop(0, 4, combine, 0)

    def square_sum(b, _):
        rows = pl.ds(pl.multiple_of(b * 128, 128), 128)
        acc = jnp.zeros((128, 128), f32)
        for q in range(4):
            v = comb[rows, q * 128 : (q + 1) * 128]
            acc = acc + v * v
        ns_buf[:, rows] = jnp.sum(acc.T.reshape(16, 8, 128), axis=0)
        return 0

    lax.fori_loop(0, 6, square_sum, 0)
    n_copies = []
    for d in range(1, 4):
        cp = pltpu.make_async_remote_copy(
            src_ref=ns_buf, dst_ref=ns_recv.at[d - 1], send_sem=n_send.at[d - 1],
            recv_sem=n_recv.at[d - 1], device_id=(ep, (x + d) % 4), device_id_type=MESH,
        )
        cp.start()
        n_copies.append(cp)
    for cp in n_copies:
        cp.wait()

    def finish(b, _):
        rows = pl.ds(pl.multiple_of(b * 128, 128), 128)
        total = ns_buf[:, rows] + ns_recv[0, :, rows] + ns_recv[1, :, rows] + ns_recv[2, :, rows]
        total = jnp.sum(total, axis=0, keepdims=True)
        scale = lax.rsqrt(total * (1.0 / D) + EPS)
        scale = jnp.broadcast_to(scale, (128, 128)).T
        for q in range(4):
            cols = slice(q * 128, (q + 1) * 128)
            out_ref[rows, cols] = (comb[rows, cols] * scale * og_ref[:, cols]).astype(bf16)
        return 0

    lax.fori_loop(0, 6, finish, 0)

    @pl.when(far_parity == 0)
    def _():
        arrived(s_buf, 27 * HALF, s_send)

    @pl.when(far_parity == 1)
    def _():
        arrived(s_buf, 25 * HALF, s_send)


    arrived(y_buf, 63 * HALF, y_send)


def per_device(
    tokens, in_gain, route_ids, route_scores, gate_weight, up_weight, down_weight, out_gain
):
    vmem = pl.BlockSpec(memory_space=pltpu.VMEM)
    hbm = pl.BlockSpec(memory_space=pl.ANY)
    dma = pltpu.SemaphoreType.DMA
    return pl.pallas_call(
        kernel,
        out_shape=jax.ShapeDtypeStruct((T, DQ), bf16),
        in_specs=[hbm, vmem, vmem, vmem, hbm, hbm, hbm, vmem],
        out_specs=vmem,
        scratch_shapes=[
            pltpu.VMEM((T, D), bf16),
            pltpu.VMEM((4 * ROWS, D), bf16),
            pltpu.VMEM((4 * ROWS, D), bf16),
            pltpu.VMEM((2, D, F), bf16),
            pltpu.VMEM((2, D, F), bf16),
            pltpu.VMEM((4 * F, 2 * DQ), bf16),
            pltpu.VMEM((8, ROWS // 2, 2 * F), bf16),
            pltpu.VMEM((8, ROWS // 2, 2 * F), bf16),
            pltpu.VMEM((64 * HALF, DQ), bf16),
            pltpu.VMEM((64 * HALF, DQ), bf16),
            pltpu.VMEM((128, T), f32),
            pltpu.VMEM((T, 128), bf16),
            pltpu.VMEM((T, T), bf16),
            pltpu.VMEM((T, 128), f32),
            pltpu.VMEM((T, 128), f32),
            pltpu.VMEM((T, 128), f32),
            pltpu.VMEM((T, 128), f32),
            pltpu.VMEM((T, 128), f32),
            pltpu.VMEM((T, DQ), f32),
            pltpu.VMEM((8, T), f32),
            pltpu.VMEM((3, 8, T), f32),
            dma((5,)),
            dma,
            dma((4,)),
            dma,
            dma,
            dma((5,)),
            dma((5,)),
            dma((8,)),
            dma((8,)),
            dma,
            dma((4,)),
            dma((3,)),
            dma((3,)),
            pltpu.SemaphoreType.REGULAR,
        ],
        compiler_params=pltpu.CompilerParams(
            collective_id=0, has_side_effects=True, vmem_limit_bytes=62 * 2**20
        ),
        name="routed_experts",
    )(
        tokens,
        in_gain.reshape(1, D),
        route_ids.T,
        route_scores.T,
        gate_weight.reshape(D, F),
        up_weight.reshape(D, F),
        down_weight.reshape(F, D),
        out_gain.reshape(1, DQ),
    )


def solution(mesh):
    in_specs = (
        P("ep", None),
        P(),
        P("ep", None),
        P("ep", None),
        P("ep", None, "tp"),
        P("ep", None, "tp"),
        P("ep", "tp", None),
        P("tp"),
    )
    return jax.shard_map(
        per_device, mesh=mesh, in_specs=in_specs, out_specs=P("ep", "tp"), check_vma=False
    )
```

```python
import jax
import jax.numpy as jnp
from jax import lax
from jax.experimental import pallas as pl
from jax.experimental.pallas import tpu as pltpu
from jax.sharding import PartitionSpec as P

EPS = 1e-06
MESH = pl.DeviceIdType.MESH
T = 768
D = 2048
F = 256
CAP = 96
HALF = 48
ROWS = 4 * 2 * HALF
DQ = 512
STEPS = (
    (1, 2), (3, 2), (2, 1), (2, 3),
    (2, 2), (0, 1), (0, 3), (2, 0),
    (1, 1), (3, 3), (0, 2), (1, 0),
    (1, 3), (3, 1), (3, 0), (0, 0),
)
FAR = 5
OWN = 3 * 8 + 3
f32 = jnp.float32
bf16 = jnp.bfloat16


def dot(a, b):
    return jnp.dot(a, b, preferred_element_type=f32)


def at_rows(ref, start, size):
    return ref.at[pl.ds(pl.multiple_of(start, 16), size), :]


def kernel(
    tok_hbm, gain_hbm, ids_hbm, score_hbm, wg_hbm, wu_hbm, wd_hbm,
    comb,
    gain_ref, ids_ref, score_ref,
    tok, s_buf, x_buf, wg, wu, wd, h_buf, h_recv, y_buf, r_buf,
    slot_t, onehot, sel, col0, col1, mix0, mix1, rowsum, ns_buf, ns_recv,
    local_sem, s_send, x_recv, f_send, f_recv, w_send, w_recv, h_send, h_rsem, y_send, r_recv, n_send, n_recv, ready,
):
    ep = lax.axis_index("ep")
    x = lax.axis_index("tp")
    z = ep // 8
    y = (ep // 2) % 4
    c = ep % 2
    xs = (x - c + 5) % 4
    half = xs // 2
    member = xs % 2
    x_gate = ((((x - c + 4) % 4) + 1 - 2 * (((x - c + 4) % 4) % 2)) + c) % 4
    x_hid = (xs + 1 - 2 * member + c + 3) % 4
    x_far = (x + 2) % 4

    def peer(p, dc, sign):
        dz, dy = STEPS[p]
        return (
            ((z + sign * dz + 4) % 4) * 8 + ((y + sign * dy + 4) % 4) * 2 + (c + dc) % 2
        )

    small_copies = [
        pltpu.make_async_copy(a, b, local_sem.at[5 + i])
        for i, (a, b) in enumerate(
            ((ids_hbm, ids_ref), (score_hbm, score_ref), (gain_hbm, gain_ref))
        )
    ]
    for cp in small_copies:
        cp.start()
    tok_copy = pltpu.make_async_copy(tok_hbm, tok, local_sem.at[0])
    tok_copy.start()
    wg_copy = pltpu.make_async_copy(wg_hbm, wg.at[0], local_sem.at[1])
    wu_copy = pltpu.make_async_copy(wu_hbm, wu.at[0], local_sem.at[2])

    def features(k):
        return pl.ds(pl.multiple_of(k * DQ, DQ), DQ)

    def shard(k, part):
        return wd.at[pl.ds(k * F, F), pl.ds(part * DQ, DQ)]

    wd_copies = [
        pltpu.make_async_copy(wd_hbm.at[:, features(k)], shard(0, q), local_sem.at[3 + q])
        for q, k in enumerate((x, x_gate))
    ]
    wg_copy.start()
    wu_copy.start()
    for cp in wd_copies:
        cp.start()

    barrier = pltpu.get_barrier_semaphore()

    def greet(i, _):
        pl.semaphore_signal(
            barrier, inc=1, device_id=((ep + i) % 32, x), device_id_type=MESH
        )
        return 0

    lax.fori_loop(1, 32, greet, 0)
    for d in range(1, 4):
        pl.semaphore_signal(
            barrier, inc=1, device_id=(ep, (x + d) % 4), device_id_type=MESH
        )

    for cp in small_copies:
        cp.wait()

    lanes = lax.broadcasted_iota(jnp.int32, (128, 128), 1)
    dz_l = ((lanes >> 3) - z) & 3
    dy_l = (((lanes >> 1) & 3) - y) & 3
    dc_l = ((lanes & 1) - c) & 1
    base = dc_l * (4 * CAP)
    for p, (dz, dy) in enumerate(STEPS):
        base = base + jnp.where(
            dz_l * 4 + dy_l == dz * 4 + dy, (p // 4 * 8 + p % 4) * CAP, 0
        )
    base = base.astype(f32)
    lanes_f = lanes.astype(f32)

    def column(row):
        return jnp.broadcast_to(row, (128, 128)).T

    def mark(b, _):
        rows = pl.ds(pl.multiple_of(b * 128, 128), 128)
        first = column(ids_ref[0:1, rows].astype(f32))
        second = column(ids_ref[1:2, rows].astype(f32))
        col0[rows, :] = first
        col1[rows, :] = second
        named = (first == lanes_f) | (second == lanes_f)
        onehot[rows, :] = jnp.where(named, 1.0, 0.0).astype(bf16)
        score0 = score_ref[0:1, rows]
        score1 = score_ref[1:2, rows]
        mix0[rows, :] = column(score0 / (score0 + score1))
        mix1[rows, :] = column(score1 / (score0 + score1))
        return 0

    lax.fori_loop(0, 6, mark, 0)

    def number(b, _):
        rows = pl.ds(pl.multiple_of(b * 128, 128), 128)
        earlier = lax.broadcasted_iota(jnp.int32, (128, T), 1) < (
            lax.broadcasted_iota(jnp.int32, (128, T), 0) + b * 128
        )
        count = dot(jnp.where(earlier, 1.0, 0.0).astype(bf16), onehot[...])
        first = col0[rows, :] == lanes_f
        second = col1[rows, :] == lanes_f
        slot_t[:, rows] = jnp.where(first | second, count, -1.0).T
        place = count + base
        col0[rows, :] = jnp.broadcast_to(
            jnp.sum(jnp.where(first, place, 0.0), axis=1, keepdims=True), (128, 128)
        )
        col1[rows, :] = jnp.broadcast_to(
            jnp.sum(jnp.where(second, place, 0.0), axis=1, keepdims=True), (128, 128)
        )
        return 0

    lax.fori_loop(0, 6, number, 0)

    tok_copy.wait()

    def squares(b, _):
        rows = pl.ds(pl.multiple_of(b * 64, 64), 64)
        acc = jnp.zeros((64, 128), f32)
        for q in range(16):
            v = tok[rows, q * 128 : (q + 1) * 128].astype(f32)
            acc = acc + v * v
        rowsum[rows, :] = acc
        return 0

    lax.fori_loop(0, 12, squares, 0)

    def scale_of(b, _):
        rows = pl.ds(pl.multiple_of(b * 256, 256), 256)
        mean = jnp.sum(rowsum[rows, :], axis=1, keepdims=True) * (1.0 / D)
        rowsum[rows, :] = jnp.broadcast_to(lax.rsqrt(mean + EPS), (256, 128))
        return 0

    lax.fori_loop(0, 3, scale_of, 0)

    def normalize(b, _):
        rows = pl.ds(pl.multiple_of(b * 64, 64), 64)
        scale = rowsum[rows, :]
        for q in range(16):
            cols = slice(q * 128, (q + 1) * 128)
            v = tok[rows, cols].astype(f32) * scale * gain_ref[:, cols]
            tok[rows, cols] = v.astype(bf16)
        return 0

    lax.fori_loop(0, 12, normalize, 0)

    def pack(g):
        for q in range(8):
            dc, j = q // 4, q % 4
            e = peer(g * 4 + j, dc, 1)
            first = ((x - (c + dc) % 2 + 5) % 4) // 2 * HALF
            want = lax.broadcasted_iota(jnp.int32, (HALF, T), 0) + first
            row = slot_t[pl.ds(e, 1), :]
            sel[q * HALF : (q + 1) * HALF, :] = jnp.where(
                row == want.astype(f32), 1.0, 0.0
            ).astype(bf16)
        rows = slice(g * ROWS, (g + 1) * ROWS)

        def part(n, _):
            cols = pl.ds(pl.multiple_of(n * 512, 512), 512)
            s_buf[rows, cols] = dot(sel[0:ROWS, :], tok[:, cols]).astype(bf16)
            return 0

        lax.fori_loop(0, 4, part, 0)

    far_parity = (x + c + 1) % 2

    def dispatch(steps):
        def one(n, _):
            k, dc = n // 2, n % 2
            for p in steps:
                if p == 15:
                    go = dc > 0
                elif p < FAR:
                    go = far_parity == p % 2
                else:
                    go = dc >= 0

                @pl.when(go)
                def _():
                    row = (p // 4 * 8 + dc * 4 + p % 4) * HALF + k * 16
                    pltpu.make_async_remote_copy(
                        src_ref=at_rows(s_buf, row, 16), dst_ref=at_rows(x_buf, row, 16),
                        send_sem=s_send, recv_sem=x_recv.at[0 if p < FAR else p // 4],
                        device_id=(peer(p, dc, 1), x), device_id_type=MESH,
                    ).start()

            return 0

        lax.fori_loop(0, 6, one, 0)

    def send_weight(src, dst, to, sem):
        cp = pltpu.make_async_remote_copy(
            src_ref=src, dst_ref=dst, send_sem=w_send.at[sem], recv_sem=w_recv.at[sem],
            device_id=(ep, to), device_id_type=MESH,
        )
        cp.start()
        return cp

    pack(0)
    pl.semaphore_wait(barrier, 34)
    w_copies = [
        send_weight(wg_hbm, wg.at[1], x_gate, 0),
        send_weight(wu_hbm, wu.at[1], x_gate, 1),
    ]
    for k, to, parts in ((2, x_hid, (x_hid, x_far)), (1, x_gate, (x_gate, x))):
        for q in range(2):
            pltpu.make_async_remote_copy(
                src_ref=wd_hbm.at[:, features(parts[q])], dst_ref=shard(k, q),
                send_sem=w_send.at[1 + k], recv_sem=w_recv.at[1 + k],
                device_id=(ep, to), device_id_type=MESH,
            ).start()
    dispatch(range(4))
    for d in range(1, 4):
        pl.semaphore_signal(
            ready, inc=1, device_id=(ep, (x + d) % 4), device_id_type=MESH
        )
    pack(1)
    dispatch(range(4, 8))
    pack(2)
    dispatch(range(8, 12))
    pack(3)
    dispatch(range(12, 16))
    own = slice(OWN * HALF, (OWN + 1) * HALF)
    x_buf[own, :] = s_buf[own, :]

    def arrived(ref, rows, sem):
        part = ref.at[pl.ds(0, rows), :]
        pltpu.make_async_copy(part, part, sem).wait()

    def shard_copied(k):
        part = wd.at[pl.ds(k * F, F), :]
        for sem in (w_send, w_recv):
            pltpu.make_async_copy(part, part, sem.at[1 + k]).wait()

    def relay():
        shard_copied(2)
        for q in range(2):
            pltpu.make_async_remote_copy(
                src_ref=shard(2, 1 - q), dst_ref=shard(3, q),
                send_sem=w_send.at[4], recv_sem=w_recv.at[4],
                device_id=(ep, x_gate), device_id_type=MESH,
            ).start()

    def hand(p):
        row = (p // 4 * 8 + (member + p) % 2 * 4 + p % 4) * HALF
        return pltpu.make_async_remote_copy(
            src_ref=at_rows(x_buf, row, HALF), dst_ref=at_rows(x_buf, row, HALF),
            send_sem=f_send, recv_sem=f_recv,
            device_id=(ep, x_hid), device_id_type=MESH,
        )

    arrived(x_buf, FAR * HALF, x_recv.at[0])
    for p in range(FAR):
        hand(p).start()

    wg_copy.wait()
    wu_copy.wait()
    for cp in wd_copies:
        cp.wait()
    for cp in w_copies:
        cp.wait()
    relay()

    def swap(k):
        return pltpu.make_async_remote_copy(
            src_ref=h_buf.at[k], dst_ref=h_recv.at[k],
            send_sem=h_send.at[k], recv_sem=h_rsem.at[k],
            device_id=(ep, x_hid), device_id_type=MESH,
        )

    def block(k):
        return pl.ds(pl.multiple_of(k * (ROWS // 2), ROWS // 2), ROWS // 2)

    def hidden(g):
        def side(i, _):
            k = g * 2 + i
            for q in range(2):
                gate = dot(x_buf[block(k), :], wg[q])
                up = dot(x_buf[block(k), :], wu[q])
                h_buf[k, :, q * F : (q + 1) * F] = (
                    gate / (1.0 + jnp.exp(-gate)) * up
                ).astype(bf16)
            swap(k).start()
            return 0

        lax.fori_loop(0, 2, side, 0)

    def down(k):
        swap(k).wait()
        for q in range(2):
            cols = slice(q * DQ, (q + 1) * DQ)
            v = dot(h_buf[k], wd[0 : 2 * F, cols])
            v = v + dot(h_recv[k], wd[2 * F : 4 * F, cols])
            y_buf[block(k * 2 + q), :] = v.astype(bf16)

    def give(g, side):
        k = g * 2 + side
        for n in range(8):
            j, q = n % 4, (n // 4 + n) % 2
            src = ((k * 2 + q) * 4 + j) * HALF
            dst = ((k * 4 + j) * 2 + half) * HALF

            def one():
                pltpu.make_async_remote_copy(
                    src_ref=at_rows(y_buf, src, HALF), dst_ref=at_rows(r_buf, dst, HALF),
                    send_sem=y_send, recv_sem=r_recv.at[g],
                    device_id=(peer(g * 4 + j, side, -1), (x, x_gate)[q]),
                    device_id_type=MESH,
                ).start()

            if (g, j, q) == (3, 3, 0):
                pl.when(side > 0)(one)
            else:
                one()

    def finish_group(g):
        def one(side, _):
            down(g * 2 + side)
            give(g, side)
            return 0

        lax.fori_loop(0, 2, one, 0)

    arrived(x_buf, (8 - FAR) * 2 * HALF, x_recv.at[1])
    for sem in (f_send, f_recv):
        arrived(x_buf, FAR * HALF, sem)
    hidden(1)
    hidden(0)
    shard_copied(1)
    shard_copied(3)
    pl.semaphore_wait(ready, 3)
    finish_group(1)
    arrived(x_buf, ROWS, x_recv.at[2])
    hidden(2)
    finish_group(0)
    arrived(x_buf, ROWS - HALF, x_recv.at[3])
    hidden(3)
    finish_group(2)
    finish_group(3)
    r_buf[pl.ds(pl.multiple_of((OWN * 2 + half) * HALF, 16), HALF), :] = y_buf[
        (12 * 4 + 3) * HALF : (12 * 4 + 4) * HALF, :
    ]

    comb[...] = jnp.zeros_like(comb)

    def combine(i, _):
        g = i + (1 - 2 * (i % 2)) * (1 - i // 2)

        def weigh(b, _):
            rows = pl.ds(pl.multiple_of(b * 128, 128), 128)
            for q in range(6):
                here = (lanes + (g * 8 * CAP + q * 128)).astype(f32)
                v = jnp.where(col0[rows, :] == here, mix0[rows, :], 0.0)
                v = v + jnp.where(col1[rows, :] == here, mix1[rows, :], 0.0)
                sel[rows, q * 128 : (q + 1) * 128] = v.astype(bf16)
            return 0

        lax.fori_loop(0, 6, weigh, 0)

        @pl.when(g < 3)
        def _():
            arrived(r_buf, 16 * HALF, r_recv.at[g])

        @pl.when(g == 3)
        def _():
            arrived(r_buf, 15 * HALF, r_recv.at[g])

        rows = pl.ds(pl.multiple_of(g * 8 * CAP, 8 * CAP), 8 * CAP)
        comb[...] += dot(sel[...], r_buf[rows, :])
        return 0

    lax.fori_loop(0, 4, combine, 0)

    def square_sum(b, _):
        rows = pl.ds(pl.multiple_of(b * 128, 128), 128)
        acc = jnp.zeros((128, 128), f32)
        for q in range(4):
            v = comb[rows, q * 128 : (q + 1) * 128]
            acc = acc + v * v
        ns_buf[:, rows] = jnp.sum(acc.T.reshape(16, 8, 128), axis=0)
        return 0

    lax.fori_loop(0, 6, square_sum, 0)
    n_copies = []
    for d in range(1, 4):
        cp = pltpu.make_async_remote_copy(
            src_ref=ns_buf, dst_ref=ns_recv.at[d - 1], send_sem=n_send.at[d - 1],
            recv_sem=n_recv.at[d - 1], device_id=(ep, (x + d) % 4), device_id_type=MESH,
        )
        cp.start()
        n_copies.append(cp)
    for cp in n_copies:
        cp.wait()

    def finish(b, _):
        rows = pl.ds(pl.multiple_of(b * 128, 128), 128)
        total = ns_buf[:, rows] + ns_recv[0, :, rows] + ns_recv[1, :, rows] + ns_recv[2, :, rows]
        total = jnp.sum(total, axis=0, keepdims=True)
        scale = lax.rsqrt(total * (1.0 / D) + EPS)
        scale = jnp.broadcast_to(scale, (128, 128)).T
        for q in range(4):
            cols = slice(q * 128, (q + 1) * 128)
            comb[rows, cols] = comb[rows, cols] * scale
        return 0

    lax.fori_loop(0, 6, finish, 0)

    @pl.when(far_parity == 0)
    def _():
        arrived(s_buf, 27 * HALF, s_send)

    @pl.when(far_parity == 1)
    def _():
        arrived(s_buf, 25 * HALF, s_send)


    arrived(y_buf, 63 * HALF, y_send)


def per_device(
    tokens, in_gain, route_ids, route_scores, gate_weight, up_weight, down_weight, out_gain
):
    vmem = pl.BlockSpec(memory_space=pltpu.VMEM)
    hbm = pl.BlockSpec(memory_space=pl.ANY)
    dma = pltpu.SemaphoreType.DMA
    scaled = pl.pallas_call(
        kernel,
        out_shape=jax.ShapeDtypeStruct((T, DQ), f32),
        in_specs=[hbm] * 7,
        out_specs=vmem,
        scratch_shapes=[
            pltpu.VMEM((1, D), f32),
            pltpu.VMEM((2, T), jnp.int32),
            pltpu.VMEM((2, T), f32),
            pltpu.VMEM((T, D), bf16),
            pltpu.VMEM((4 * ROWS, D), bf16),
            pltpu.VMEM((4 * ROWS, D), bf16),
            pltpu.VMEM((2, D, F), bf16),
            pltpu.VMEM((2, D, F), bf16),
            pltpu.VMEM((4 * F, 2 * DQ), bf16),
            pltpu.VMEM((8, ROWS // 2, 2 * F), bf16),
            pltpu.VMEM((8, ROWS // 2, 2 * F), bf16),
            pltpu.VMEM((64 * HALF, DQ), bf16),
            pltpu.VMEM((64 * HALF, DQ), bf16),
            pltpu.VMEM((128, T), f32),
            pltpu.VMEM((T, 128), bf16),
            pltpu.VMEM((T, T), bf16),
            pltpu.VMEM((T, 128), f32),
            pltpu.VMEM((T, 128), f32),
            pltpu.VMEM((T, 128), f32),
            pltpu.VMEM((T, 128), f32),
            pltpu.VMEM((T, 128), f32),
            pltpu.VMEM((8, T), f32),
            pltpu.VMEM((3, 8, T), f32),
            dma((8,)),
            dma,
            dma((4,)),
            dma,
            dma,
            dma((5,)),
            dma((5,)),
            dma((8,)),
            dma((8,)),
            dma,
            dma((4,)),
            dma((3,)),
            dma((3,)),
            pltpu.SemaphoreType.REGULAR,
        ],
        compiler_params=pltpu.CompilerParams(
            collective_id=0, has_side_effects=True, vmem_limit_bytes=62 * 2**20
        ),
        name="routed_experts",
    )(
        tokens,
        in_gain.reshape(1, D),
        route_ids.T,
        route_scores.T,
        gate_weight.reshape(D, F),
        up_weight.reshape(D, F),
        down_weight.reshape(F, D),
    )
    return (scaled * out_gain).astype(bf16)


def solution(mesh):
    in_specs = (
        P("ep", None),
        P(),
        P("ep", None),
        P("ep", None),
        P("ep", None, "tp"),
        P("ep", None, "tp"),
        P("ep", "tp", None),
        P("tp"),
    )
    return jax.shard_map(
        per_device, mesh=mesh, in_specs=in_specs, out_specs=P("ep", "tp"), check_vma=False
    )
```

```python
import jax
import jax.numpy as jnp
from jax import lax
from jax.experimental import pallas as pl
from jax.experimental.pallas import tpu as pltpu
from jax.sharding import PartitionSpec as P

EPS = 1e-06
MESH = pl.DeviceIdType.MESH
T = 768
D = 2048
F = 256
CAP = 96
HALF = 48
ROWS = 4 * 2 * HALF
DQ = 512
STEPS = (
    (1, 2), (3, 2), (2, 1), (2, 3),
    (2, 2), (0, 1), (0, 3), (2, 0),
    (1, 1), (3, 3), (0, 2), (1, 0),
    (1, 3), (3, 1), (3, 0), (0, 0),
)
FAR = 5
OWN = 3 * 8 + 3
f32 = jnp.float32
bf16 = jnp.bfloat16


def dot(a, b):
    return jnp.dot(a, b, preferred_element_type=f32)


def at_rows(ref, start, size):
    return ref.at[pl.ds(pl.multiple_of(start, 16), size), :]


def kernel(
    tok_hbm, gain_hbm, ids_hbm, score_hbm, wg_hbm, wu_hbm, wd_hbm, og_hbm,
    out_ref,
    gain_ref, ids_ref, score_ref, og_ref,
    tok, s_buf, x_buf, wg, wu, wd, h_buf, h_recv, y_buf, r_buf,
    slot_t, onehot, sel, col0, col1, mix0, mix1, rowsum, comb, ns_buf, ns_recv,
    local_sem, s_send, x_recv, f_send, f_recv, w_send, w_recv, h_send, h_rsem, y_send, r_recv, n_send, n_recv, ready,
):
    ep = lax.axis_index("ep")
    x = lax.axis_index("tp")
    z = ep // 8
    y = (ep // 2) % 4
    c = ep % 2
    xs = (x - c + 5) % 4
    half = xs // 2
    member = xs % 2
    x_gate = ((((x - c + 4) % 4) + 1 - 2 * (((x - c + 4) % 4) % 2)) + c) % 4
    x_hid = (xs + 1 - 2 * member + c + 3) % 4
    x_far = (x + 2) % 4

    def peer(p, dc, sign):
        dz, dy = STEPS[p]
        return (
            ((z + sign * dz + 4) % 4) * 8 + ((y + sign * dy + 4) % 4) * 2 + (c + dc) % 2
        )

    small_copies = [
        pltpu.make_async_copy(a, b, local_sem.at[5 + i])
        for i, (a, b) in enumerate(
            ((ids_hbm, ids_ref), (score_hbm, score_ref), (gain_hbm, gain_ref), (og_hbm, og_ref))
        )
    ]
    for cp in small_copies:
        cp.start()
    tok_copy = pltpu.make_async_copy(tok_hbm, tok, local_sem.at[0])
    tok_copy.start()
    wg_copy = pltpu.make_async_copy(wg_hbm, wg.at[0], local_sem.at[1])
    wu_copy = pltpu.make_async_copy(wu_hbm, wu.at[0], local_sem.at[2])

    def features(k):
        return pl.ds(pl.multiple_of(k * DQ, DQ), DQ)

    def shard(k, part):
        return wd.at[pl.ds(k * F, F), pl.ds(part * DQ, DQ)]

    wd_copies = [
        pltpu.make_async_copy(wd_hbm.at[:, features(k)], shard(0, q), local_sem.at[3 + q])
        for q, k in enumerate((x, x_gate))
    ]
    wg_copy.start()
    wu_copy.start()
    for cp in wd_copies:
        cp.start()

    barrier = pltpu.get_barrier_semaphore()

    def greet(i, _):
        pl.semaphore_signal(
            barrier, inc=1, device_id=((ep + i) % 32, x), device_id_type=MESH
        )
        return 0

    lax.fori_loop(1, 32, greet, 0)
    for d in range(1, 4):
        pl.semaphore_signal(
            barrier, inc=1, device_id=(ep, (x + d) % 4), device_id_type=MESH
        )

    for cp in small_copies:
        cp.wait()

    lanes = lax.broadcasted_iota(jnp.int32, (128, 128), 1)
    dz_l = ((lanes >> 3) - z) & 3
    dy_l = (((lanes >> 1) & 3) - y) & 3
    dc_l = ((lanes & 1) - c) & 1
    base = dc_l * (4 * CAP)
    for p, (dz, dy) in enumerate(STEPS):
        base = base + jnp.where(
            dz_l * 4 + dy_l == dz * 4 + dy, (p // 4 * 8 + p % 4) * CAP, 0
        )
    base = base.astype(f32)
    lanes_f = lanes.astype(f32)

    def column(row):
        return jnp.broadcast_to(row, (128, 128)).T

    def mark(b, _):
        rows = pl.ds(pl.multiple_of(b * 128, 128), 128)
        first = column(ids_ref[0:1, rows].astype(f32))
        second = column(ids_ref[1:2, rows].astype(f32))
        col0[rows, :] = first
        col1[rows, :] = second
        named = (first == lanes_f) | (second == lanes_f)
        onehot[rows, :] = jnp.where(named, 1.0, 0.0).astype(bf16)
        score0 = score_ref[0:1, rows]
        score1 = score_ref[1:2, rows]
        mix0[rows, :] = column(score0 / (score0 + score1))
        mix1[rows, :] = column(score1 / (score0 + score1))
        return 0

    lax.fori_loop(0, 6, mark, 0)

    def number(b, _):
        rows = pl.ds(pl.multiple_of(b * 128, 128), 128)
        earlier = lax.broadcasted_iota(jnp.int32, (128, T), 1) < (
            lax.broadcasted_iota(jnp.int32, (128, T), 0) + b * 128
        )
        count = dot(jnp.where(earlier, 1.0, 0.0).astype(bf16), onehot[...])
        first = col0[rows, :] == lanes_f
        second = col1[rows, :] == lanes_f
        slot_t[:, rows] = jnp.where(first | second, count, -1.0).T
        place = count + base
        col0[rows, :] = jnp.broadcast_to(
            jnp.sum(jnp.where(first, place, 0.0), axis=1, keepdims=True), (128, 128)
        )
        col1[rows, :] = jnp.broadcast_to(
            jnp.sum(jnp.where(second, place, 0.0), axis=1, keepdims=True), (128, 128)
        )
        return 0

    lax.fori_loop(0, 6, number, 0)

    tok_copy.wait()

    def squares(b, _):
        rows = pl.ds(pl.multiple_of(b * 64, 64), 64)
        acc = jnp.zeros((64, 128), f32)
        for q in range(16):
            v = tok[rows, q * 128 : (q + 1) * 128].astype(f32)
            acc = acc + v * v
        rowsum[rows, :] = acc
        return 0

    lax.fori_loop(0, 12, squares, 0)

    def scale_of(b, _):
        rows = pl.ds(pl.multiple_of(b * 256, 256), 256)
        mean = jnp.sum(rowsum[rows, :], axis=1, keepdims=True) * (1.0 / D)
        rowsum[rows, :] = jnp.broadcast_to(lax.rsqrt(mean + EPS), (256, 128))
        return 0

    lax.fori_loop(0, 3, scale_of, 0)

    def normalize(b, _):
        rows = pl.ds(pl.multiple_of(b * 64, 64), 64)
        scale = rowsum[rows, :]
        for q in range(16):
            cols = slice(q * 128, (q + 1) * 128)
            v = tok[rows, cols].astype(f32) * scale * gain_ref[:, cols]
            tok[rows, cols] = v.astype(bf16)
        return 0

    lax.fori_loop(0, 12, normalize, 0)

    def pack(g):
        for q in range(8):
            dc, j = q // 4, q % 4
            e = peer(g * 4 + j, dc, 1)
            first = ((x - (c + dc) % 2 + 5) % 4) // 2 * HALF
            want = lax.broadcasted_iota(jnp.int32, (HALF, T), 0) + first
            row = slot_t[pl.ds(e, 1), :]
            sel[q * HALF : (q + 1) * HALF, :] = jnp.where(
                row == want.astype(f32), 1.0, 0.0
            ).astype(bf16)
        rows = slice(g * ROWS, (g + 1) * ROWS)

        def part(n, _):
            cols = pl.ds(pl.multiple_of(n * 512, 512), 512)
            s_buf[rows, cols] = dot(sel[0:ROWS, :], tok[:, cols]).astype(bf16)
            return 0

        lax.fori_loop(0, 4, part, 0)

    far_parity = (x + c + 1) % 2

    def dispatch(steps):
        def one(n, _):
            k, dc = n // 2, n % 2
            for p in steps:
                if p == 15:
                    go = dc > 0
                elif p < FAR:
                    go = far_parity == p % 2
                else:
                    go = dc >= 0

                @pl.when(go)
                def _():
                    row = (p // 4 * 8 + dc * 4 + p % 4) * HALF + k * 16
                    pltpu.make_async_remote_copy(
                        src_ref=at_rows(s_buf, row, 16), dst_ref=at_rows(x_buf, row, 16),
                        send_sem=s_send, recv_sem=x_recv.at[0 if p < FAR else p // 4],
                        device_id=(peer(p, dc, 1), x), device_id_type=MESH,
                    ).start()

            return 0

        lax.fori_loop(0, 6, one, 0)

    def send_weight(src, dst, to, sem):
        cp = pltpu.make_async_remote_copy(
            src_ref=src, dst_ref=dst, send_sem=w_send.at[sem], recv_sem=w_recv.at[sem],
            device_id=(ep, to), device_id_type=MESH,
        )
        cp.start()
        return cp

    pack(0)
    pl.semaphore_wait(barrier, 34)
    w_copies = [
        send_weight(wg_hbm, wg.at[1], x_gate, 0),
        send_weight(wu_hbm, wu.at[1], x_gate, 1),
    ]
    for k, to, parts in ((2, x_hid, (x_hid, x_far)), (1, x_gate, (x_gate, x))):
        for q in range(2):
            pltpu.make_async_remote_copy(
                src_ref=wd_hbm.at[:, features(parts[q])], dst_ref=shard(k, q),
                send_sem=w_send.at[1 + k], recv_sem=w_recv.at[1 + k],
                device_id=(ep, to), device_id_type=MESH,
            ).start()
    dispatch(range(4))
    for d in range(1, 4):
        pl.semaphore_signal(
            ready, inc=1, device_id=(ep, (x + d) % 4), device_id_type=MESH
        )
    pack(1)
    dispatch(range(4, 8))
    pack(2)
    dispatch(range(8, 12))
    pack(3)
    dispatch(range(12, 16))
    own = slice(OWN * HALF, (OWN + 1) * HALF)
    x_buf[own, :] = s_buf[own, :]

    def arrived(ref, rows, sem):
        part = ref.at[pl.ds(0, rows), :]
        pltpu.make_async_copy(part, part, sem).wait()

    def shard_copied(k):
        part = wd.at[pl.ds(k * F, F), :]
        for sem in (w_send, w_recv):
            pltpu.make_async_copy(part, part, sem.at[1 + k]).wait()

    def relay():
        shard_copied(2)
        for q in range(2):
            pltpu.make_async_remote_copy(
                src_ref=shard(2, 1 - q), dst_ref=shard(3, q),
                send_sem=w_send.at[4], recv_sem=w_recv.at[4],
                device_id=(ep, x_gate), device_id_type=MESH,
            ).start()

    def hand(p):
        row = (p // 4 * 8 + (member + p) % 2 * 4 + p % 4) * HALF
        return pltpu.make_async_remote_copy(
            src_ref=at_rows(x_buf, row, HALF), dst_ref=at_rows(x_buf, row, HALF),
            send_sem=f_send, recv_sem=f_recv,
            device_id=(ep, x_hid), device_id_type=MESH,
        )

    arrived(x_buf, FAR * HALF, x_recv.at[0])
    for p in range(FAR):
        hand(p).start()

    wg_copy.wait()
    wu_copy.wait()
    for cp in wd_copies:
        cp.wait()
    for cp in w_copies:
        cp.wait()
    relay()

    def swap(k):
        return pltpu.make_async_remote_copy(
            src_ref=h_buf.at[k], dst_ref=h_recv.at[k],
            send_sem=h_send.at[k], recv_sem=h_rsem.at[k],
            device_id=(ep, x_hid), device_id_type=MESH,
        )

    def block(k):
        return pl.ds(pl.multiple_of(k * (ROWS // 2), ROWS // 2), ROWS // 2)

    def hidden(g):
        def side(i, _):
            k = g * 2 + i
            for q in range(2):
                gate = dot(x_buf[block(k), :], wg[q])
                up = dot(x_buf[block(k), :], wu[q])
                h_buf[k, :, q * F : (q + 1) * F] = (
                    gate / (1.0 + jnp.exp(-gate)) * up
                ).astype(bf16)
            swap(k).start()
            return 0

        lax.fori_loop(0, 2, side, 0)

    def down(k):
        swap(k).wait()
        for q in range(2):
            cols = slice(q * DQ, (q + 1) * DQ)
            v = dot(h_buf[k], wd[0 : 2 * F, cols])
            v = v + dot(h_recv[k], wd[2 * F : 4 * F, cols])
            y_buf[block(k * 2 + q), :] = v.astype(bf16)

    def give(g, side):
        k = g * 2 + side
        for n in range(8):
            j, q = n % 4, (n // 4 + n) % 2
            src = ((k * 2 + q) * 4 + j) * HALF
            dst = ((k * 4 + j) * 2 + half) * HALF

            def one():
                pltpu.make_async_remote_copy(
                    src_ref=at_rows(y_buf, src, HALF), dst_ref=at_rows(r_buf, dst, HALF),
                    send_sem=y_send, recv_sem=r_recv.at[g],
                    device_id=(peer(g * 4 + j, side, -1), (x, x_gate)[q]),
                    device_id_type=MESH,
                ).start()

            if (g, j, q) == (3, 3, 0):
                pl.when(side > 0)(one)
            else:
                one()

    def finish_group(g):
        def one(side, _):
            down(g * 2 + side)
            give(g, side)
            return 0

        lax.fori_loop(0, 2, one, 0)

    arrived(x_buf, (8 - FAR) * 2 * HALF, x_recv.at[1])
    for sem in (f_send, f_recv):
        arrived(x_buf, FAR * HALF, sem)
    hidden(1)
    hidden(0)
    shard_copied(1)
    shard_copied(3)
    pl.semaphore_wait(ready, 3)
    finish_group(1)
    arrived(x_buf, ROWS, x_recv.at[2])
    hidden(2)
    finish_group(0)
    arrived(x_buf, ROWS - HALF, x_recv.at[3])
    hidden(3)
    finish_group(2)
    finish_group(3)
    r_buf[pl.ds(pl.multiple_of((OWN * 2 + half) * HALF, 16), HALF), :] = y_buf[
        (12 * 4 + 3) * HALF : (12 * 4 + 4) * HALF, :
    ]

    comb[...] = jnp.zeros_like(comb)

    def combine(i, _):
        g = i + (1 - 2 * (i % 2)) * (1 - i // 2)

        def weigh(b, _):
            rows = pl.ds(pl.multiple_of(b * 128, 128), 128)
            for q in range(6):
                here = (lanes + (g * 8 * CAP + q * 128)).astype(f32)
                v = jnp.where(col0[rows, :] == here, mix0[rows, :], 0.0)
                v = v + jnp.where(col1[rows, :] == here, mix1[rows, :], 0.0)
                sel[rows, q * 128 : (q + 1) * 128] = v.astype(bf16)
            return 0

        lax.fori_loop(0, 6, weigh, 0)

        @pl.when(g < 3)
        def _():
            arrived(r_buf, 16 * HALF, r_recv.at[g])

        @pl.when(g == 3)
        def _():
            arrived(r_buf, 15 * HALF, r_recv.at[g])

        rows = pl.ds(pl.multiple_of(g * 8 * CAP, 8 * CAP), 8 * CAP)
        comb[...] += dot(sel[...], r_buf[rows, :])
        return 0

    lax.fori_loop(0, 4, combine, 0)

    def square_sum(b, _):
        rows = pl.ds(pl.multiple_of(b * 128, 128), 128)
        acc = jnp.zeros((128, 128), f32)
        for q in range(4):
            v = comb[rows, q * 128 : (q + 1) * 128]
            acc = acc + v * v
        ns_buf[:, rows] = jnp.sum(acc.T.reshape(16, 8, 128), axis=0)
        return 0

    lax.fori_loop(0, 6, square_sum, 0)
    n_copies = []
    for d in range(1, 4):
        cp = pltpu.make_async_remote_copy(
            src_ref=ns_buf, dst_ref=ns_recv.at[d - 1], send_sem=n_send.at[d - 1],
            recv_sem=n_recv.at[d - 1], device_id=(ep, (x + d) % 4), device_id_type=MESH,
        )
        cp.start()
        n_copies.append(cp)
    for cp in n_copies:
        cp.wait()

    def finish(b, _):
        rows = pl.ds(pl.multiple_of(b * 128, 128), 128)
        total = ns_buf[:, rows] + ns_recv[0, :, rows] + ns_recv[1, :, rows] + ns_recv[2, :, rows]
        total = jnp.sum(total, axis=0, keepdims=True)
        scale = lax.rsqrt(total * (1.0 / D) + EPS)
        scale = jnp.broadcast_to(scale, (128, 128)).T
        for q in range(4):
            cols = slice(q * 128, (q + 1) * 128)
            out_ref[rows, cols] = (comb[rows, cols] * scale * og_ref[:, cols]).astype(bf16)
        return 0

    lax.fori_loop(0, 6, finish, 0)

    @pl.when(far_parity == 0)
    def _():
        arrived(s_buf, 27 * HALF, s_send)

    @pl.when(far_parity == 1)
    def _():
        arrived(s_buf, 25 * HALF, s_send)


    arrived(y_buf, 63 * HALF, y_send)


def per_device(
    tokens, in_gain, route_ids, route_scores, gate_weight, up_weight, down_weight, out_gain
):
    vmem = pl.BlockSpec(memory_space=pltpu.VMEM)
    hbm = pl.BlockSpec(memory_space=pl.ANY)
    dma = pltpu.SemaphoreType.DMA
    return pl.pallas_call(
        kernel,
        out_shape=jax.ShapeDtypeStruct((T, DQ), bf16),
        in_specs=[hbm] * 8,
        out_specs=vmem,
        scratch_shapes=[
            pltpu.VMEM((1, D), f32),
            pltpu.VMEM((2, T), jnp.int32),
            pltpu.VMEM((2, T), f32),
            pltpu.VMEM((1, DQ), f32),
            pltpu.VMEM((T, D), bf16),
            pltpu.VMEM((4 * ROWS, D), bf16),
            pltpu.VMEM((4 * ROWS, D), bf16),
            pltpu.VMEM((2, D, F), bf16),
            pltpu.VMEM((2, D, F), bf16),
            pltpu.VMEM((4 * F, 2 * DQ), bf16),
            pltpu.VMEM((8, ROWS // 2, 2 * F), bf16),
            pltpu.VMEM((8, ROWS // 2, 2 * F), bf16),
            pltpu.VMEM((64 * HALF, DQ), bf16),
            pltpu.VMEM((64 * HALF, DQ), bf16),
            pltpu.VMEM((128, T), f32),
            pltpu.VMEM((T, 128), bf16),
            pltpu.VMEM((T, T), bf16),
            pltpu.VMEM((T, 128), f32),
            pltpu.VMEM((T, 128), f32),
            pltpu.VMEM((T, 128), f32),
            pltpu.VMEM((T, 128), f32),
            pltpu.VMEM((T, 128), f32),
            pltpu.VMEM((T, DQ), f32),
            pltpu.VMEM((8, T), f32),
            pltpu.VMEM((3, 8, T), f32),
            dma((9,)),
            dma,
            dma((4,)),
            dma,
            dma,
            dma((5,)),
            dma((5,)),
            dma((8,)),
            dma((8,)),
            dma,
            dma((4,)),
            dma((3,)),
            dma((3,)),
            pltpu.SemaphoreType.REGULAR,
        ],
        compiler_params=pltpu.CompilerParams(
            collective_id=0, has_side_effects=True, vmem_limit_bytes=62 * 2**20
        ),
        name="routed_experts",
    )(
        tokens,
        in_gain.reshape(1, D),
        route_ids.T,
        route_scores.T,
        gate_weight.reshape(D, F),
        up_weight.reshape(D, F),
        down_weight.reshape(F, D),
        out_gain.reshape(1, DQ),
    )


def solution(mesh):
    in_specs = (
        P("ep", None),
        P(),
        P("ep", None),
        P("ep", None),
        P("ep", None, "tp"),
        P("ep", None, "tp"),
        P("ep", "tp", None),
        P("tp"),
    )
    return jax.shard_map(
        per_device, mesh=mesh, in_specs=in_specs, out_specs=P("ep", "tp"), check_vma=False
    )
```

```python
import jax
import jax.numpy as jnp
from jax import lax
from jax.experimental import pallas as pl
from jax.experimental.pallas import tpu as pltpu
from jax.sharding import PartitionSpec as P

EPS = 1e-06
MESH = pl.DeviceIdType.MESH
T = 768
D = 2048
F = 256
CAP = 96
HALF = 48
ROWS = 4 * 2 * HALF
DQ = 512
STEPS = (
    (1, 2), (3, 2), (2, 1), (2, 3),
    (2, 2), (0, 1), (0, 3), (2, 0),
    (1, 1), (3, 3), (0, 2), (1, 0),
    (1, 3), (3, 1), (3, 0), (0, 0),
)
FAR = 5
OWN = 3 * 8 + 3
f32 = jnp.float32
bf16 = jnp.bfloat16


def dot(a, b):
    return jnp.dot(a, b, preferred_element_type=f32)


def at_rows(ref, start, size):
    return ref.at[pl.ds(pl.multiple_of(start, 16), size), :]


def kernel(
    tok_hbm, gain_hbm, ids_hbm, score_hbm, wg_hbm, wu_hbm, wd_hbm, og_hbm,
    out_ref,
    gain_ref, ids_ref, score_ref, og_ref,
    tok, s_buf, x_buf, wg, wu, wd, h_buf, h_recv, y_buf, r_buf,
    slot_t, onehot, sel, col0, col1, mix0, mix1, rowsum, comb, ns_buf, ns_recv,
    local_sem, s_send, x_recv, f_send, f_recv, w_send, w_recv, h_send, h_rsem, y_send, r_recv, n_send, n_recv, ready,
):
    ep = lax.axis_index("ep")
    x = lax.axis_index("tp")
    z = ep // 8
    y = (ep // 2) % 4
    c = ep % 2
    xs = (x - c + 5) % 4
    half = xs // 2
    member = xs % 2
    x_gate = ((((x - c + 4) % 4) + 1 - 2 * (((x - c + 4) % 4) % 2)) + c) % 4
    x_hid = (xs + 1 - 2 * member + c + 3) % 4
    x_far = (x + 2) % 4

    def peer(p, dc, sign):
        dz, dy = STEPS[p]
        return (
            ((z + sign * dz + 4) % 4) * 8 + ((y + sign * dy + 4) % 4) * 2 + (c + dc) % 2
        )

    small_copies = [
        pltpu.make_async_copy(a, b, local_sem.at[5 + i])
        for i, (a, b) in enumerate(
            ((ids_hbm, ids_ref), (score_hbm, score_ref), (gain_hbm, gain_ref), (og_hbm, og_ref))
        )
    ]
    for cp in small_copies:
        cp.start()
    tok_copy = pltpu.make_async_copy(tok_hbm, tok, local_sem.at[0])
    tok_copy.start()
    wg_copy = pltpu.make_async_copy(wg_hbm, wg.at[0], local_sem.at[1])
    wu_copy = pltpu.make_async_copy(wu_hbm, wu.at[0], local_sem.at[2])

    def features(k):
        return pl.ds(pl.multiple_of(k * DQ, DQ), DQ)

    def shard(k, part):
        return wd.at[pl.ds(k * F, F), pl.ds(part * DQ, DQ)]

    wd_copies = [
        pltpu.make_async_copy(wd_hbm.at[:, features(k)], shard(0, q), local_sem.at[3 + q])
        for q, k in enumerate((x, x_gate))
    ]
    wg_copy.start()
    wu_copy.start()
    for cp in wd_copies:
        cp.start()

    barrier = pltpu.get_barrier_semaphore()

    def greet(i, _):
        pl.semaphore_signal(
            barrier, inc=1, device_id=((ep + i) % 32, x), device_id_type=MESH
        )
        return 0

    lax.fori_loop(1, 32, greet, 0)
    for d in range(1, 4):
        pl.semaphore_signal(
            barrier, inc=1, device_id=(ep, (x + d) % 4), device_id_type=MESH
        )

    for cp in small_copies:
        cp.wait()

    lanes = lax.broadcasted_iota(jnp.int32, (128, 128), 1)
    dz_l = ((lanes >> 3) - z) & 3
    dy_l = (((lanes >> 1) & 3) - y) & 3
    dc_l = ((lanes & 1) - c) & 1
    base = dc_l * (4 * CAP)
    for p, (dz, dy) in enumerate(STEPS):
        base = base + jnp.where(
            dz_l * 4 + dy_l == dz * 4 + dy, (p // 4 * 8 + p % 4) * CAP, 0
        )
    base = base.astype(f32)
    lanes_f = lanes.astype(f32)

    def column(row):
        return jnp.broadcast_to(row, (128, 128)).T

    def mark(b, _):
        rows = pl.ds(pl.multiple_of(b * 128, 128), 128)
        first = column(ids_ref[0:1, rows].astype(f32))
        second = column(ids_ref[1:2, rows].astype(f32))
        col0[rows, :] = first
        col1[rows, :] = second
        named = (first == lanes_f) | (second == lanes_f)
        onehot[rows, :] = jnp.where(named, 1.0, 0.0).astype(bf16)
        score0 = score_ref[0:1, rows]
        score1 = score_ref[1:2, rows]
        mix0[rows, :] = column(score0 / (score0 + score1))
        mix1[rows, :] = column(score1 / (score0 + score1))
        return 0

    lax.fori_loop(0, 6, mark, 0)

    def number(b, _):
        rows = pl.ds(pl.multiple_of(b * 128, 128), 128)
        earlier = lax.broadcasted_iota(jnp.int32, (128, T), 1) < (
            lax.broadcasted_iota(jnp.int32, (128, T), 0) + b * 128
        )
        count = dot(jnp.where(earlier, 1.0, 0.0).astype(bf16), onehot[...])
        first = col0[rows, :] == lanes_f
        second = col1[rows, :] == lanes_f
        slot_t[:, rows] = jnp.where(first | second, count, -1.0).T
        place = count + base
        col0[rows, :] = jnp.broadcast_to(
            jnp.sum(jnp.where(first, place, 0.0), axis=1, keepdims=True), (128, 128)
        )
        col1[rows, :] = jnp.broadcast_to(
            jnp.sum(jnp.where(second, place, 0.0), axis=1, keepdims=True), (128, 128)
        )
        return 0

    lax.fori_loop(0, 6, number, 0)

    tok_copy.wait()

    def squares(b, _):
        rows = pl.ds(pl.multiple_of(b * 64, 64), 64)
        acc = jnp.zeros((64, 128), f32)
        for q in range(16):
            v = tok[rows, q * 128 : (q + 1) * 128].astype(f32)
            acc = acc + v * v
        rowsum[rows, :] = acc
        return 0

    lax.fori_loop(0, 12, squares, 0)

    def scale_of(b, _):
        rows = pl.ds(pl.multiple_of(b * 256, 256), 256)
        mean = jnp.sum(rowsum[rows, :], axis=1, keepdims=True) * (1.0 / D)
        rowsum[rows, :] = jnp.broadcast_to(lax.rsqrt(mean + EPS), (256, 128))
        return 0

    lax.fori_loop(0, 3, scale_of, 0)

    def normalize(b, _):
        rows = pl.ds(pl.multiple_of(b * 64, 64), 64)
        scale = rowsum[rows, :]
        for q in range(16):
            cols = slice(q * 128, (q + 1) * 128)
            v = tok[rows, cols].astype(f32) * scale * gain_ref[:, cols]
            tok[rows, cols] = v.astype(bf16)
        return 0

    lax.fori_loop(0, 12, normalize, 0)

    def pack(g):
        for q in range(8):
            dc, j = q // 4, q % 4
            e = peer(g * 4 + j, dc, 1)
            first = ((x - (c + dc) % 2 + 5) % 4) // 2 * HALF
            want = lax.broadcasted_iota(jnp.int32, (HALF, T), 0) + first
            row = slot_t[pl.ds(e, 1), :]
            sel[q * HALF : (q + 1) * HALF, :] = jnp.where(
                row == want.astype(f32), 1.0, 0.0
            ).astype(bf16)
        rows = slice(g * ROWS, (g + 1) * ROWS)

        def part(n, _):
            cols = pl.ds(pl.multiple_of(n * 512, 512), 512)
            s_buf[rows, cols] = dot(sel[0:ROWS, :], tok[:, cols]).astype(bf16)
            return 0

        lax.fori_loop(0, 4, part, 0)

    far_parity = (x + c + 1) % 2

    def dispatch(steps):
        def one(n, _):
            k, dc = n // 2, n % 2
            for p in steps:
                if p == 15:
                    go = dc > 0
                elif p < FAR:
                    go = far_parity == p % 2
                else:
                    go = dc >= 0

                @pl.when(go)
                def _():
                    row = (p // 4 * 8 + dc * 4 + p % 4) * HALF + k * 16
                    pltpu.make_async_remote_copy(
                        src_ref=at_rows(s_buf, row, 16), dst_ref=at_rows(x_buf, row, 16),
                        send_sem=s_send, recv_sem=x_recv.at[0 if p < FAR else p // 4],
                        device_id=(peer(p, dc, 1), x), device_id_type=MESH,
                    ).start()

            return 0

        lax.fori_loop(0, 6, one, 0)

    def send_weight(src, dst, to, sem):
        cp = pltpu.make_async_remote_copy(
            src_ref=src, dst_ref=dst, send_sem=w_send.at[sem], recv_sem=w_recv.at[sem],
            device_id=(ep, to), device_id_type=MESH,
        )
        cp.start()
        return cp

    pack(0)
    pl.semaphore_wait(barrier, 34)
    w_copies = [
        send_weight(wg_hbm, wg.at[1], x_gate, 0),
        send_weight(wu_hbm, wu.at[1], x_gate, 1),
    ]
    for k, to, parts in ((2, x_hid, (x_hid, x_far)), (1, x_gate, (x_gate, x))):
        for q in range(2):
            pltpu.make_async_remote_copy(
                src_ref=wd_hbm.at[:, features(parts[q])], dst_ref=shard(k, q),
                send_sem=w_send.at[1 + k], recv_sem=w_recv.at[1 + k],
                device_id=(ep, to), device_id_type=MESH,
            ).start()
    dispatch(range(4))
    for d in range(1, 4):
        pl.semaphore_signal(
            ready, inc=1, device_id=(ep, (x + d) % 4), device_id_type=MESH
        )
    pack(1)
    dispatch(range(4, 8))
    pack(2)
    dispatch(range(8, 12))
    pack(3)
    dispatch(range(12, 16))
    own = slice(OWN * HALF, (OWN + 1) * HALF)
    x_buf[own, :] = s_buf[own, :]

    def arrived(ref, rows, sem):
        part = ref.at[pl.ds(0, rows), :]
        pltpu.make_async_copy(part, part, sem).wait()

    def shard_copied(k):
        part = wd.at[pl.ds(k * F, F), :]
        for sem in (w_send, w_recv):
            pltpu.make_async_copy(part, part, sem.at[1 + k]).wait()

    def relay():
        shard_copied(2)
        for q in range(2):
            pltpu.make_async_remote_copy(
                src_ref=shard(2, 1 - q), dst_ref=shard(3, q),
                send_sem=w_send.at[4], recv_sem=w_recv.at[4],
                device_id=(ep, x_gate), device_id_type=MESH,
            ).start()

    def hand(p):
        row = (p // 4 * 8 + (member + p) % 2 * 4 + p % 4) * HALF
        return pltpu.make_async_remote_copy(
            src_ref=at_rows(x_buf, row, HALF), dst_ref=at_rows(x_buf, row, HALF),
            send_sem=f_send, recv_sem=f_recv,
            device_id=(ep, x_hid), device_id_type=MESH,
        )

    arrived(x_buf, FAR * HALF, x_recv.at[0])
    for p in reversed(range(FAR)):
        hand(p).start()

    wg_copy.wait()
    wu_copy.wait()
    for cp in wd_copies:
        cp.wait()
    for cp in w_copies:
        cp.wait()
    relay()

    def swap(k):
        return pltpu.make_async_remote_copy(
            src_ref=h_buf.at[k], dst_ref=h_recv.at[k],
            send_sem=h_send.at[k], recv_sem=h_rsem.at[k],
            device_id=(ep, x_hid), device_id_type=MESH,
        )

    def block(k):
        return pl.ds(pl.multiple_of(k * (ROWS // 2), ROWS // 2), ROWS // 2)

    def hidden(g):
        def side(i, _):
            k = g * 2 + i
            for q in range(2):
                gate = dot(x_buf[block(k), :], wg[q])
                up = dot(x_buf[block(k), :], wu[q])
                h_buf[k, :, q * F : (q + 1) * F] = (
                    gate / (1.0 + jnp.exp(-gate)) * up
                ).astype(bf16)
            swap(k).start()
            return 0

        lax.fori_loop(0, 2, side, 0)

    def down(k):
        swap(k).wait()
        for q in range(2):
            cols = slice(q * DQ, (q + 1) * DQ)
            v = dot(h_buf[k], wd[0 : 2 * F, cols])
            v = v + dot(h_recv[k], wd[2 * F : 4 * F, cols])
            y_buf[block(k * 2 + q), :] = v.astype(bf16)

    def give(g, side):
        k = g * 2 + side
        for n in range(8):
            j, q = n % 4, (n // 4 + n) % 2
            src = ((k * 2 + q) * 4 + j) * HALF
            dst = ((k * 4 + j) * 2 + half) * HALF

            def one():
                pltpu.make_async_remote_copy(
                    src_ref=at_rows(y_buf, src, HALF), dst_ref=at_rows(r_buf, dst, HALF),
                    send_sem=y_send, recv_sem=r_recv.at[g],
                    device_id=(peer(g * 4 + j, side, -1), (x, x_gate)[q]),
                    device_id_type=MESH,
                ).start()

            if (g, j, q) == (3, 3, 0):
                pl.when(side > 0)(one)
            else:
                one()

    def finish_group(g):
        def one(side, _):
            down(g * 2 + side)
            give(g, side)
            return 0

        lax.fori_loop(0, 2, one, 0)

    arrived(x_buf, (8 - FAR) * 2 * HALF, x_recv.at[1])
    for sem in (f_send, f_recv):
        arrived(x_buf, FAR * HALF, sem)
    hidden(1)
    hidden(0)
    shard_copied(1)
    shard_copied(3)
    pl.semaphore_wait(ready, 3)
    finish_group(1)
    arrived(x_buf, ROWS, x_recv.at[2])
    hidden(2)
    finish_group(0)
    arrived(x_buf, ROWS - HALF, x_recv.at[3])
    hidden(3)
    finish_group(2)
    finish_group(3)
    r_buf[pl.ds(pl.multiple_of((OWN * 2 + half) * HALF, 16), HALF), :] = y_buf[
        (12 * 4 + 3) * HALF : (12 * 4 + 4) * HALF, :
    ]

    comb[...] = jnp.zeros_like(comb)

    def combine(i, _):
        g = i + (1 - 2 * (i % 2)) * (1 - i // 2)

        def weigh(b, _):
            rows = pl.ds(pl.multiple_of(b * 128, 128), 128)
            for q in range(6):
                here = (lanes + (g * 8 * CAP + q * 128)).astype(f32)
                v = jnp.where(col0[rows, :] == here, mix0[rows, :], 0.0)
                v = v + jnp.where(col1[rows, :] == here, mix1[rows, :], 0.0)
                sel[rows, q * 128 : (q + 1) * 128] = v.astype(bf16)
            return 0

        lax.fori_loop(0, 6, weigh, 0)

        @pl.when(g < 3)
        def _():
            arrived(r_buf, 16 * HALF, r_recv.at[g])

        @pl.when(g == 3)
        def _():
            arrived(r_buf, 15 * HALF, r_recv.at[g])

        rows = pl.ds(pl.multiple_of(g * 8 * CAP, 8 * CAP), 8 * CAP)
        comb[...] += dot(sel[...], r_buf[rows, :])
        return 0

    lax.fori_loop(0, 4, combine, 0)

    def square_sum(b, _):
        rows = pl.ds(pl.multiple_of(b * 128, 128), 128)
        acc = jnp.zeros((128, 128), f32)
        for q in range(4):
            v = comb[rows, q * 128 : (q + 1) * 128]
            acc = acc + v * v
        ns_buf[:, rows] = jnp.sum(acc.T.reshape(16, 8, 128), axis=0)
        return 0

    lax.fori_loop(0, 6, square_sum, 0)
    n_copies = []
    for d in range(1, 4):
        cp = pltpu.make_async_remote_copy(
            src_ref=ns_buf, dst_ref=ns_recv.at[d - 1], send_sem=n_send.at[d - 1],
            recv_sem=n_recv.at[d - 1], device_id=(ep, (x + d) % 4), device_id_type=MESH,
        )
        cp.start()
        n_copies.append(cp)
    for cp in n_copies:
        cp.wait()

    def finish(b, _):
        rows = pl.ds(pl.multiple_of(b * 128, 128), 128)
        total = ns_buf[:, rows] + ns_recv[0, :, rows] + ns_recv[1, :, rows] + ns_recv[2, :, rows]
        total = jnp.sum(total, axis=0, keepdims=True)
        scale = lax.rsqrt(total * (1.0 / D) + EPS)
        scale = jnp.broadcast_to(scale, (128, 128)).T
        for q in range(4):
            cols = slice(q * 128, (q + 1) * 128)
            out_ref[rows, cols] = (comb[rows, cols] * scale * og_ref[:, cols]).astype(bf16)
        return 0

    lax.fori_loop(0, 6, finish, 0)

    @pl.when(far_parity == 0)
    def _():
        arrived(s_buf, 27 * HALF, s_send)

    @pl.when(far_parity == 1)
    def _():
        arrived(s_buf, 25 * HALF, s_send)


    arrived(y_buf, 63 * HALF, y_send)


def per_device(
    tokens, in_gain, route_ids, route_scores, gate_weight, up_weight, down_weight, out_gain
):
    vmem = pl.BlockSpec(memory_space=pltpu.VMEM)
    hbm = pl.BlockSpec(memory_space=pl.ANY)
    dma = pltpu.SemaphoreType.DMA
    return pl.pallas_call(
        kernel,
        out_shape=jax.ShapeDtypeStruct((T, DQ), bf16),
        in_specs=[hbm] * 8,
        out_specs=vmem,
        scratch_shapes=[
            pltpu.VMEM((1, D), f32),
            pltpu.VMEM((2, T), jnp.int32),
            pltpu.VMEM((2, T), f32),
            pltpu.VMEM((1, DQ), f32),
            pltpu.VMEM((T, D), bf16),
            pltpu.VMEM((4 * ROWS, D), bf16),
            pltpu.VMEM((4 * ROWS, D), bf16),
            pltpu.VMEM((2, D, F), bf16),
            pltpu.VMEM((2, D, F), bf16),
            pltpu.VMEM((4 * F, 2 * DQ), bf16),
            pltpu.VMEM((8, ROWS // 2, 2 * F), bf16),
            pltpu.VMEM((8, ROWS // 2, 2 * F), bf16),
            pltpu.VMEM((64 * HALF, DQ), bf16),
            pltpu.VMEM((64 * HALF, DQ), bf16),
            pltpu.VMEM((128, T), f32),
            pltpu.VMEM((T, 128), bf16),
            pltpu.VMEM((T, T), bf16),
            pltpu.VMEM((T, 128), f32),
            pltpu.VMEM((T, 128), f32),
            pltpu.VMEM((T, 128), f32),
            pltpu.VMEM((T, 128), f32),
            pltpu.VMEM((T, 128), f32),
            pltpu.VMEM((T, DQ), f32),
            pltpu.VMEM((8, T), f32),
            pltpu.VMEM((3, 8, T), f32),
            dma((9,)),
            dma,
            dma((4,)),
            dma,
            dma,
            dma((5,)),
            dma((5,)),
            dma((8,)),
            dma((8,)),
            dma,
            dma((4,)),
            dma((3,)),
            dma((3,)),
            pltpu.SemaphoreType.REGULAR,
        ],
        compiler_params=pltpu.CompilerParams(
            collective_id=0, has_side_effects=True, vmem_limit_bytes=62 * 2**20
        ),
        name="routed_experts",
    )(
        tokens,
        in_gain.reshape(1, D),
        route_ids.T,
        route_scores.T,
        gate_weight.reshape(D, F),
        up_weight.reshape(D, F),
        down_weight.reshape(F, D),
        out_gain.reshape(1, DQ),
    )


def solution(mesh):
    in_specs = (
        P("ep", None),
        P(),
        P("ep", None),
        P("ep", None),
        P("ep", None, "tp"),
        P("ep", None, "tp"),
        P("ep", "tp", None),
        P("tp"),
    )
    return jax.shard_map(
        per_device, mesh=mesh, in_specs=in_specs, out_specs=P("ep", "tp"), check_vma=False
    )
```
